32 devices in a mesh: grp: 2 (over x), ep: 16 (over z, y, core).
Axes of the slice: x: 2, y: 2, z: 4, core: 2. Of those that a mesh axis runs over, the one named last changes fastest.
Arguments:
- tokens: bfloat16 [128, 2048], P(('grp', 'ep')), parts along dimension 0, may hold values from -6 to 6
- lengths: int32 [128], P(('grp', 'ep')), parts along dimension 0, may hold values from 128 to 1024, as said below
- cache_key: bfloat16 [128, 1024, 256], P(('grp', 'ep')), parts along dimension 0, may hold values from -6 to 6
- cache_value: bfloat16 [128, 1024, 256], P(('grp', 'ep')), parts along dimension 0, may hold values from -6 to 6
- routes: int32 [128, 2], P(('grp', 'ep')), parts along dimension 0, may hold values from 0 to 3, all different within a row
- route_logits: float32 [128, 2], P(('grp', 'ep')), parts along dimension 0, may hold values from -6 to 6
- mix_gain: float32 [2048], replicated, may hold values from 0.1 to 1.9
- query_gain: float32 [64], replicated, may hold values from 0.1 to 1.9
- key_gain: float32 [64], replicated, may hold values from 0.1 to 1.9
- head_bias: float32 [16], replicated, may hold values from -9 to -3.5
- w_query: bfloat16 [2048, 1024], P('ep'), may hold values from -0.125 to 0.125
- w_key: bfloat16 [2048, 256], P('ep'), may hold values from -0.125 to 0.125
- w_value: bfloat16 [2048, 256], P('ep'), may hold values from -0.125 to 0.125
- w_out: bfloat16 [1024, 2048], P(None, 'ep'), may hold values from -0.1875 to 0.1875
- ffn_gain: float32 [2048], replicated, may hold values from 0.1 to 1.9
- w_gate: bfloat16 [2048, 28672], P(None, 'ep'), may hold values from -0.125 to 0.125
- w_up: bfloat16 [2048, 28672], P(None, 'ep'), may hold values from -0.125 to 0.125
- w_down: bfloat16 [28672, 2048], P('ep'), may hold values from -0.0625 to 0.0625
Outputs:
- output: bfloat16 [128, 2048], P(('grp', 'ep')), parts along dimension 0
- new_key: bfloat16 [128, 256], P(('grp', 'ep')), parts along dimension 0
- new_value: bfloat16 [128, 256], P(('grp', 'ep')), parts along dimension 0
The draws below stay inside these ranges and needn't reach their ends.
There are 2 independent parts, one for each index of `grp`. The reference program is written for one: setup_inputs(seed, part) draws one part's arguments, and reference() takes and returns one part's arrays. A program takes and returns all parts, laid end to end along the dimension named above; an argument that names none is the same for every part. Nothing has to cross between parts.
Inputs may be any that keep to these rules, and one draw needn't show every extreme that they name: `lengths`: some sequence has all 1024 positions live.
All inputs are finite; a program needn't handle non-finite values.
Results may differ from the reference program's by a relative error of at most 0.0085.
Values may be sent and summed in bfloat16 or wider, within the bound.
No kernel may reach another device: no remote copies, remote signals or barrier semaphores. Data moves between devices by JAX's collectives and lax.ppermute only.
A program may use at most 128 MiB of HBM per device.

```python
import jax
import jax.numpy as jnp
from jax import lax

D = 2048
HEADS = 16
KV_HEADS = 4
HEAD_DIM = 64
FF = 7168
EXPERTS = 4
TOP = 2
CACHE_LEN = 1024
BATCH = 64


def draw_lengths(key, part):
    spread = jax.random.randint(key, (BATCH,), CACHE_LEN // 8, CACHE_LEN + 1)
    chosen = jax.random.randint(jax.random.fold_in(key, 7), (), 0, BATCH)
    return jnp.where(jnp.arange(BATCH) == chosen, CACHE_LEN, spread).astype(jnp.int32)


def draw_head_bias(key, part):
    picker = jax.random.uniform(jax.random.fold_in(key, 1), (HEADS,), jnp.float32)
    quick = jax.random.uniform(jax.random.fold_in(key, 2), (HEADS,), jnp.float32, -4.5, -3.5)
    steady = jax.random.uniform(jax.random.fold_in(key, 3), (HEADS,), jnp.float32, -9.0, -7.5)
    portion = 0.5
    return jnp.where(picker < portion, quick, steady).astype(jnp.float32)


def steps_of(rng, dims, split, low, top_value):
    level, own = 1.0, jax.random.fold_in(rng, 6)
    for dim, parts in split:
        steps = jnp.exp(jax.random.uniform(jax.random.fold_in(own, dim), (parts,), jnp.float32, low / len(split), top_value / len(split)))
        level = level * jnp.repeat(steps, dims[dim] // parts).reshape([-1 if axis == dim else 1 for axis in range(len(dims))])
    return level


def distinct(key, rows, number_of, top, lift):
    ranking = jax.random.permutation(jax.random.fold_in(key, 1), number_of)
    favour = ranking
    for power in range(3):
        favour = favour * favour // number_of
    favour = favour * lift // number_of
    tickets = jax.random.randint(jax.random.fold_in(key, 2), (rows, number_of), 0, 4096) + favour
    fixed_rows = jax.random.permutation(jax.random.fold_in(key, 3), rows)[jnp.arange(number_of) % rows]
    tickets = jnp.where(jnp.arange(rows)[:, None] == fixed_rows[None, :], 1 << 14, tickets)
    priority = tickets * number_of + jnp.arange(number_of)
    return lax.top_k(priority.astype(jnp.int32), top)[1].astype(jnp.int32)


def normal_values(rng, dims, scale, bound, cuts=(), held_as=jnp.bfloat16):
    entries = scale * jax.random.normal(rng, dims, jnp.float32)
    if cuts:
        entries = entries * steps_of(rng, dims, cuts, -0.22, 0.18)
    return jnp.clip(entries, -bound, bound).astype(held_as)


def setup_inputs(seed: int = 0, part: int = 0) -> dict:
    arg_keys = jax.random.split(jax.random.key(seed), 19)
    part_keys = jax.random.split(jax.random.fold_in(arg_keys[18], part), 19)
    return {
        "tokens": normal_values(part_keys[0], (BATCH, D), 1.0, 6.0, ((0, 16),)),
        "lengths": draw_lengths(jax.random.fold_in(jax.random.fold_in(arg_keys[18], part), 71), part),
        "cache_key": normal_values(part_keys[2], (BATCH, CACHE_LEN, KV_HEADS * HEAD_DIM), 1.0, 6.0, ((0, 16),)),
        "cache_value": normal_values(part_keys[3], (BATCH, CACHE_LEN, KV_HEADS * HEAD_DIM), 1.0, 6.0, ((0, 16),)),
        "routes": distinct(part_keys[4], BATCH, EXPERTS, TOP, 4096),
        "route_logits": normal_values(part_keys[5], (BATCH, TOP), 1.5, 6.0, ((0, 16),), jnp.float32),
        "mix_gain": jnp.clip(1.0 + 0.18 * jax.random.normal(arg_keys[6], (D,), jnp.float32), 0.1, 1.9),
        "query_gain": jnp.clip(1.0 + 0.18 * jax.random.normal(arg_keys[7], (HEAD_DIM,), jnp.float32), 0.1, 1.9),
        "key_gain": jnp.clip(1.0 + 0.18 * jax.random.normal(arg_keys[8], (HEAD_DIM,), jnp.float32), 0.1, 1.9),
        "head_bias": draw_head_bias(jax.random.fold_in(arg_keys[18], 71), part),
        "w_query": normal_values(arg_keys[10], (D, HEADS * HEAD_DIM), D ** -0.5, 0.125, ((0, 16),)),
        "w_key": normal_values(arg_keys[11], (D, KV_HEADS * HEAD_DIM), D ** -0.5, 0.125, ((0, 16),)),
        "w_value": normal_values(arg_keys[12], (D, KV_HEADS * HEAD_DIM), D ** -0.5, 0.125, ((0, 16),)),
        "w_out": normal_values(arg_keys[13], (HEADS * HEAD_DIM, D), (HEADS * HEAD_DIM) ** -0.5, 0.1875, ((1, 16),)),
        "ffn_gain": jnp.clip(1.0 + 0.18 * jax.random.normal(arg_keys[14], (D,), jnp.float32), 0.1, 1.9),
        "w_gate": normal_values(arg_keys[15], (D, EXPERTS * FF), D ** -0.5, 0.125, ((1, 16),)),
        "w_up": normal_values(arg_keys[16], (D, EXPERTS * FF), D ** -0.5, 0.125, ((1, 16),)),
        "w_down": normal_values(arg_keys[17], (EXPERTS * FF, D), FF ** -0.5, 0.0625, ((0, 16),)),
    }


EPSILON = 1e-06

def rms_scaled(values, gain):
    return values * lax.rsqrt(lax.optimization_barrier(jnp.mean(values * values, axis=-1, keepdims=True)) + EPSILON) * gain

def route_weights(routes, route_logits):
    experts_iota = jnp.arange(EXPERTS, dtype=jnp.int32)[None, :]
    first_share = jax.nn.sigmoid(route_logits[:, 0:1] - route_logits[:, 1:2])
    second_share = jax.nn.sigmoid(route_logits[:, 1:2] - route_logits[:, 0:1])
    return jnp.where(routes[:, 0:1] == experts_iota, first_share, 0.0) + jnp.where(routes[:, 1:2] == experts_iota, second_share, 0.0)

def reference(tokens, lengths, cache_key, cache_value, routes, route_logits, mix_gain, query_gain, key_gain, head_bias, w_query, w_key, w_value, w_out, ffn_gain, w_gate, w_up, w_down):
    as_float = tokens.astype(jnp.float32)
    normed = rms_scaled(as_float, mix_gain).astype(jnp.bfloat16)
    queries = jnp.dot(normed, w_query, preferred_element_type=jnp.float32)
    fresh_key = jnp.dot(normed, w_key, preferred_element_type=jnp.float32)
    fresh_value = jnp.dot(normed, w_value, preferred_element_type=jnp.float32)
    batch_rows = tokens.shape[0]
    group_size = HEADS // KV_HEADS
    normed_query = rms_scaled(queries.reshape(batch_rows, HEADS, HEAD_DIM), query_gain).astype(jnp.bfloat16)
    normed_query = normed_query.reshape(batch_rows, KV_HEADS, group_size, HEAD_DIM)
    new_key = rms_scaled(fresh_key.reshape(batch_rows, KV_HEADS, HEAD_DIM), key_gain)
    new_key = new_key.reshape(batch_rows, KV_HEADS * HEAD_DIM).astype(jnp.bfloat16)
    new_value = fresh_value.astype(jnp.bfloat16)
    key_heads = cache_key.reshape(batch_rows, CACHE_LEN, KV_HEADS, HEAD_DIM).astype(jnp.float32)
    value_heads = cache_value.reshape(batch_rows, CACHE_LEN, KV_HEADS, HEAD_DIM).astype(jnp.float32)
    scores = jnp.einsum('bkgd,blkd->bkgl', normed_query.astype(jnp.float32), key_heads) * HEAD_DIM ** (-0.5)
    scores = scores + head_bias.reshape(KV_HEADS, group_size)[None, :, :, None]
    live_mask = jnp.arange(CACHE_LEN, dtype=jnp.int32)[None, None, None, :] < lengths.astype(jnp.int32)[:, None, None, None]
    remain = jnp.where(live_mask, jax.nn.log_sigmoid(-scores), 0.0)
    after_sum = lax.cumsum(remain, axis=3, reverse=True) - remain
    weights = jnp.where(live_mask, jnp.exp(jax.nn.log_sigmoid(scores) + after_sum), 0.0).astype(jnp.bfloat16)
    attended = jnp.einsum('bkgl,blkd->bkgd', weights.astype(jnp.float32), value_heads)
    attended = attended.reshape(batch_rows, HEADS * HEAD_DIM).astype(jnp.bfloat16)
    mixed = as_float + jnp.dot(attended, w_out, preferred_element_type=jnp.float32)
    expert_in = rms_scaled(mixed, ffn_gain).astype(jnp.bfloat16)
    gate_table = route_weights(routes, route_logits)
    expert_sum = jnp.zeros_like(mixed)
    for expert in range(EXPERTS):
        gate_value = jnp.dot(expert_in, w_gate[:, expert * FF:(expert + 1) * FF], preferred_element_type=jnp.float32)
        up_value = jnp.dot(expert_in, w_up[:, expert * FF:(expert + 1) * FF], preferred_element_type=jnp.float32)
        hidden = (jax.nn.silu(gate_value) * up_value * gate_table[:, expert:expert + 1]).astype(jnp.bfloat16)
        expert_sum = expert_sum + jnp.dot(hidden, w_down[expert * FF:(expert + 1) * FF], preferred_element_type=jnp.float32)
    return ((mixed + expert_sum).astype(jnp.bfloat16), new_key, new_value)
```

```python
import functools

import jax
import jax.numpy as jnp
from jax import lax
from jax.experimental import pallas as pl
from jax.experimental.pallas import tpu as pltpu
from jax.sharding import PartitionSpec as P

HEADS = 16
KV_HEADS = 4
HEAD_DIM = 64
FF = 7168
EXPERTS = 4
EPSILON = 1e-06

GROUP = HEADS // KV_HEADS
KEY_WIDTH = KV_HEADS * HEAD_DIM
QUERY_WIDTH = HEADS * HEAD_DIM
ROW_WIDTH = QUERY_WIDTH + 128
BLOCK = 256
F32 = jnp.float32
BF16 = jnp.bfloat16
VMEM = pltpu.VMEM
NT = (((1,), (1,)), ((), ()))


def vmem_spec():
    return pl.BlockSpec(memory_space=VMEM)


def smem_spec():
    return pl.BlockSpec(memory_space=pltpu.SMEM)


def project_kernel(rows_ref, gain_ref, wq_ref, wk_ref, wv_ref, out_ref):
    shards, tokens, width = rows_ref.shape
    rows = rows_ref[...].astype(F32).reshape(shards * tokens, width)
    scaled = (rows * gain_ref[...]).astype(BF16)
    start = 0
    for w_ref in (wq_ref, wk_ref, wv_ref):
        size = w_ref.shape[1]
        part = jnp.dot(scaled, w_ref[...], preferred_element_type=F32)
        out_ref[:, :, start : start + size] = part.astype(BF16).reshape(shards, tokens, size)
        start += size


def attend_kernel(
    lengths_ref,
    routes_ref,
    logits_ref,
    bias_ref,
    parts_ref,
    tokens_ref,
    qgain_ref,
    kgain_ref,
    key_ref,
    value_ref,
    row_ref,
    new_key_ref,
    new_value_ref,
    heads_scr,
):
    shards, tokens, _ = parts_ref.shape
    cache_len = key_ref.shape[1]
    columns = tokens * HEADS

    own = tokens_ref[...].astype(F32)
    token_scale = lax.rsqrt(jnp.mean(own * own, axis=-1, keepdims=True) + EPSILON)
    total = parts_ref[0].astype(F32)
    for shard in range(1, shards):
        total = total + parts_ref[shard].astype(F32)
    total = total * token_scale
    fresh_key = total[:, QUERY_WIDTH : QUERY_WIDTH + KEY_WIDTH]
    new_value_ref[...] = total[:, QUERY_WIDTH + KEY_WIDTH :].astype(BF16)

    lane = lax.broadcasted_iota(jnp.int32, (tokens, KEY_WIDTH), 1)
    squares = fresh_key * fresh_key
    key_scale = jnp.zeros_like(fresh_key)
    for head in range(KV_HEADS):
        mine = lane // HEAD_DIM == head
        mean = jnp.sum(jnp.where(mine, squares, 0.0), axis=-1, keepdims=True) / HEAD_DIM
        key_scale = jnp.where(mine, lax.rsqrt(mean + EPSILON), key_scale)
    new_key_ref[...] = (fresh_key * key_scale * kgain_ref[...]).astype(BF16)

    for member in range(GROUP):
        pieces = []
        for group in range(KV_HEADS):
            head = group * GROUP + member
            pieces.append(total[:, head * HEAD_DIM : (head + 1) * HEAD_DIM])
        heads_scr[:, member, :] = jnp.concatenate(pieces, axis=-1)
    stacked = []
    for token in range(tokens):
        stacked += [heads_scr[token]] * KV_HEADS
    query = jnp.concatenate(stacked, axis=0)
    row = lax.broadcasted_iota(jnp.int32, query.shape, 0)
    col = lax.broadcasted_iota(jnp.int32, query.shape, 1)
    query = jnp.where(row % HEADS // GROUP == col // HEAD_DIM, query, 0.0)
    query_mean = jnp.sum(query * query, axis=-1, keepdims=True) / HEAD_DIM
    query = query * lax.rsqrt(query_mean + EPSILON) * qgain_ref[...]
    query = query.astype(BF16).astype(F32)
    padded = [
        jnp.where(row // HEADS == token, query, 0.0).astype(BF16) for token in range(tokens)
    ]

    out_col = lax.broadcasted_iota(jnp.int32, (1, columns), 1)
    live = jnp.zeros((1, columns), jnp.int32)
    bias = jnp.zeros((1, columns), F32)
    for token in range(tokens):
        live = jnp.where(out_col // HEADS == token, lengths_ref[token], live)
    for head in range(HEADS):
        bias = jnp.where(out_col % HEADS == head, bias_ref[head], bias)

    upper = (
        lax.broadcasted_iota(jnp.int32, (BLOCK, BLOCK), 1)
        >= lax.broadcasted_iota(jnp.int32, (BLOCK, BLOCK), 0)
    ).astype(F32).astype(BF16)
    carry = jnp.zeros((1, columns), F32)
    attended = [jnp.zeros((HEADS, KEY_WIDTH), F32) for _ in range(tokens)]
    for block in range(cache_len // BLOCK - 1, -1, -1):
        span = slice(block * BLOCK, (block + 1) * BLOCK)
        score = lax.dot_general(key_ref[0, span, :], padded[0], NT, preferred_element_type=F32)
        for token in range(1, tokens):
            score = score + lax.dot_general(
                key_ref[token, span, :], padded[token], NT, preferred_element_type=F32
            )
        score = score * HEAD_DIM ** (-0.5) + bias
        spot = lax.broadcasted_iota(jnp.int32, score.shape, 0) + block * BLOCK
        alive = spot < live
        remain = -(jnp.maximum(score, 0.0) + jnp.log1p(jnp.exp(-jnp.abs(score))))
        remain = jnp.where(alive, remain, 0.0)
        high = remain.astype(BF16)
        low = (remain - high.astype(F32)).astype(BF16)
        inclusive = (
            jnp.dot(upper, high, preferred_element_type=F32)
            + jnp.dot(upper, low, preferred_element_type=F32)
            + carry
        )
        carry = inclusive[0:1, :]
        weight = jnp.where(alive, jnp.exp(score + inclusive), 0.0)
        weight = weight.T.astype(BF16)
        for token in range(tokens):
            attended[token] = attended[token] + jnp.dot(
                weight[token * HEADS : (token + 1) * HEADS, :],
                value_ref[token, span, :],
                preferred_element_type=F32,
            )

    own_row = lax.broadcasted_iota(jnp.int32, (HEADS, KEY_WIDTH), 0)
    own_col = lax.broadcasted_iota(jnp.int32, (HEADS, KEY_WIDTH), 1)
    keep = own_row // GROUP == own_col // HEAD_DIM
    for token in range(tokens):
        kept = jnp.where(keep, attended[token], 0.0)
        folded = kept[0:GROUP]
        for group in range(1, KV_HEADS):
            folded = folded + kept[group * GROUP : (group + 1) * GROUP]
        heads_scr[token] = folded
    for member in range(GROUP):
        piece = heads_scr[:, member, :].astype(BF16)
        for shard in range(shards):
            row_ref[shard, :, member * KEY_WIDTH : (member + 1) * KEY_WIDTH] = piece

    gate_row = lax.broadcasted_iota(jnp.int32, (tokens, 128), 0)
    gate_col = lax.broadcasted_iota(jnp.int32, (tokens, 128), 1)
    first = jnp.zeros((tokens, 128), jnp.int32)
    second = jnp.zeros((tokens, 128), jnp.int32)
    gap = jnp.zeros((tokens, 128), F32)
    for token in range(tokens):
        first = jnp.where(gate_row == token, routes_ref[0, token], first)
        second = jnp.where(gate_row == token, routes_ref[1, token], second)
        gap = jnp.where(gate_row == token, logits_ref[0, token] - logits_ref[1, token], gap)
    share = jnp.where(first == gate_col % 64, jax.nn.sigmoid(gap), 0.0)
    share = share + jnp.where(second == gate_col % 64, jax.nn.sigmoid(-gap), 0.0)
    share_high = share.astype(BF16).astype(F32)
    share = jnp.where(gate_col < 64, share_high, share - share_high).astype(BF16)
    for shard in range(shards):
        row_ref[shard, :, QUERY_WIDTH:] = share


def mix_kernel(rows_ref, tokens_ref, w_ref, mixed_ref):
    shards, tokens, width = tokens_ref.shape
    total = shards * tokens
    mixed = tokens_ref[...].astype(F32).reshape(total, width)
    rows = rows_ref[...].astype(F32).reshape(total, ROW_WIDTH).astype(BF16)
    for member in range(GROUP):
        pieces = []
        for group in range(KV_HEADS):
            head = group * GROUP + member
            pieces.append(w_ref[head * HEAD_DIM : (head + 1) * HEAD_DIM, :])
        weight = jnp.concatenate(pieces, axis=0)
        mixed = mixed + jnp.dot(
            rows[:, member * KEY_WIDTH : (member + 1) * KEY_WIDTH],
            weight,
            preferred_element_type=F32,
        )
    mixed = mixed.astype(BF16)
    for shard in range(shards):
        mixed_ref[shard] = mixed


def expert_kernel(expert_ref, mixed_ref, rows_ref, gain_ref, wg_ref, wu_ref, wd_ref, out_ref):
    total, features = mixed_ref.shape[-2], gain_ref.shape[1]
    shards, tokens = rows_ref.shape[:2]
    if len(mixed_ref.shape) == 3:
        mixed = jnp.concatenate([mixed_ref[s].astype(F32) for s in range(mixed_ref.shape[0])], axis=-1)
    else:
        mixed = mixed_ref[...].astype(F32)
    scale = lax.rsqrt(jnp.mean(mixed * mixed, axis=-1, keepdims=True) + EPSILON)
    expert_in = (mixed * scale * gain_ref[...]).astype(BF16)
    gates = rows_ref[:, :, QUERY_WIDTH:].astype(F32).reshape(total, 128)
    lane = lax.broadcasted_iota(jnp.int32, gates.shape, 1)
    gate = jnp.sum(jnp.where(lane % 64 == expert_ref[0], gates, 0.0), axis=-1, keepdims=True)
    size = wg_ref.shape[1]
    chunk = BLOCK if size % BLOCK == 0 else size
    result = jnp.zeros((total, features), F32)
    hidden = []
    for start in range(0, size, chunk):
        up = jnp.dot(expert_in, wu_ref[:, start : start + chunk], preferred_element_type=F32)
        value = jnp.dot(expert_in, wg_ref[:, start : start + chunk], preferred_element_type=F32)
        hidden.append((value / (1.0 + jnp.exp(-value)) * up * gate).astype(BF16))
    hidden = jnp.concatenate(hidden, axis=-1) if len(hidden) > 1 else hidden[0]
    for start in range(0, features, BLOCK):
        part = jnp.dot(hidden, wd_ref[:, start : start + BLOCK], preferred_element_type=F32)
        out_ref[:, :, start : start + BLOCK] = part.astype(BF16).reshape(shards, tokens, BLOCK)


def finish_kernel(parts_ref, mixed_ref, out_ref):
    total = mixed_ref[...].astype(F32)
    for shard in range(parts_ref.shape[0]):
        total = total + parts_ref[shard].astype(F32)
    out_ref[...] = total.astype(BF16)


def call(kernel, name, outs, specs, scratch=()):
    single = not isinstance(outs, tuple)
    return pl.pallas_call(
        kernel,
        name=name,
        out_shape=outs,
        in_specs=specs,
        out_specs=vmem_spec() if single else tuple(vmem_spec() for _ in outs),
        scratch_shapes=list(scratch),
        compiler_params=pltpu.CompilerParams(vmem_limit_bytes=20 << 20),
    )


def in_vmem(array):
    return pltpu.with_memory_space_constraint(array, VMEM)


def local(
    tokens,
    lengths,
    cache_key,
    cache_value,
    routes,
    route_logits,
    mix_gain,
    query_gain,
    key_gain,
    head_bias,
    w_query,
    w_key,
    w_value,
    w_out,
    ffn_gain,
    w_gate,
    w_up,
    w_down,
):
    shards = lax.axis_size("ep")
    me = lax.axis_index("ep")
    token_rows, width = tokens.shape
    share = width // shards
    all_rows = shards * token_rows
    exchange = functools.partial(lax.all_to_all, axis_name="ep", split_axis=0, concat_axis=0)
    shape = jax.ShapeDtypeStruct

    sliced = tokens.reshape(token_rows, shards, share).transpose(1, 0, 2)
    sliced = exchange(sliced)
    my_gain = lax.dynamic_slice_in_dim(mix_gain, me * share, share)[None, :]
    project_width = QUERY_WIDTH + 2 * KEY_WIDTH
    parts = call(
        project_kernel,
        "project",
        shape((shards, token_rows, project_width), BF16),
        [vmem_spec()] * 5,
    )(sliced, my_gain, w_query, w_key, w_value)
    parts = exchange(parts)

    rows, new_key, new_value = call(
        attend_kernel,
        "attend",
        (
            shape((shards, token_rows, ROW_WIDTH), BF16),
            shape((token_rows, KEY_WIDTH), BF16),
            shape((token_rows, KEY_WIDTH), BF16),
        ),
        [smem_spec()] * 4 + [vmem_spec()] * 6,
        [pltpu.VMEM((token_rows, GROUP, KEY_WIDTH), F32)],
    )(
        lengths,
        routes.T,
        route_logits.T,
        head_bias,
        parts,
        tokens,
        jnp.tile(query_gain, KV_HEADS)[None, :],
        jnp.tile(key_gain, KV_HEADS)[None, :],
        in_vmem(cache_key),
        in_vmem(cache_value),
    )
    rows = exchange(rows)

    mixed = call(
        mix_kernel,
        "mix",
        shape((shards, all_rows, share), BF16),
        [vmem_spec()] * 3,
    )(rows, sliced, w_out)
    mixed = exchange(mixed)

    ff_share = w_gate.shape[1]
    my_expert = (me // (FF // ff_share)).astype(jnp.int32).reshape(1)
    if share % 128:
        expert_rows = mixed.transpose(1, 0, 2).reshape(all_rows, width)
    else:
        expert_rows = mixed
    sums = call(
        expert_kernel,
        "expert",
        shape((shards, token_rows, width), BF16),
        [smem_spec()] + [vmem_spec()] * 6,
    )(
        my_expert,
        expert_rows,
        rows,
        ffn_gain[None, :],
        in_vmem(w_gate),
        in_vmem(w_up),
        in_vmem(w_down),
    )
    sums = exchange(sums)
    mine = lax.dynamic_slice_in_dim(mixed, me * token_rows, token_rows, 1)
    mine = mine.transpose(1, 0, 2).reshape(token_rows, width)
    output = call(
        finish_kernel, "finish", shape((token_rows, width), BF16), [vmem_spec()] * 2
    )(sums, mine)
    return output, new_key, new_value


def solution(mesh):
    return jax.shard_map(
        local,
        mesh=mesh,
        in_specs=(
            P(("grp", "ep"), None),
            P(("grp", "ep")),
            P(("grp", "ep"), None, None),
            P(("grp", "ep"), None, None),
            P(("grp", "ep"), None),
            P(("grp", "ep"), None),
            P(),
            P(),
            P(),
            P(),
            P("ep", None),
            P("ep", None),
            P("ep", None),
            P(None, "ep"),
            P(),
            P(None, "ep"),
            P(None, "ep"),
            P("ep", None),
        ),
        out_specs=(P(("grp", "ep"), None), P(("grp", "ep"), None), P(("grp", "ep"), None)),
        check_vma=False,
    )
```

```python
import functools

import jax
import jax.numpy as jnp
from jax import lax
from jax.experimental import pallas as pl
from jax.experimental.pallas import tpu as pltpu
from jax.sharding import PartitionSpec as P

HEADS = 16
KV_HEADS = 4
HEAD_DIM = 64
FF = 7168
EXPERTS = 4
EPSILON = 1e-06

GROUP = HEADS // KV_HEADS
KEY_WIDTH = KV_HEADS * HEAD_DIM
QUERY_WIDTH = HEADS * HEAD_DIM
ROW_WIDTH = QUERY_WIDTH + 128
BLOCK = 256
F32 = jnp.float32
BF16 = jnp.bfloat16
VMEM = pltpu.VMEM
NT = (((1,), (1,)), ((), ()))


def vmem_spec():
    return pl.BlockSpec(memory_space=VMEM)


def smem_spec():
    return pl.BlockSpec(memory_space=pltpu.SMEM)


def stage_kernel(
    lengths_hbm,
    routes_hbm,
    logits_hbm,
    bias_hbm,
    qgain_hbm,
    kgain_hbm,
    mix_gain_hbm,
    ffn_gain_hbm,
    tokens_hbm,
    wq_hbm,
    wk_hbm,
    wv_hbm,
    w_out_hbm,
    key_hbm,
    my_gain_ref,
    scale_ref,
    column_ref,
    head_gain_ref,
    share_ref,
    ffn_gain_ref,
    w_in_ref,
    w_out_ref,
    key_ref,
    lengths_scr,
    routes_scr,
    logits_scr,
    bias_scr,
    head_gain_scr,
    mix_gain_scr,
    tokens_scr,
    sems,
):
    tokens = tokens_hbm.shape[0]
    small = [
        (lengths_hbm, lengths_scr),
        (routes_hbm, routes_scr),
        (logits_hbm, logits_scr),
        (bias_hbm, bias_scr),
        (qgain_hbm, head_gain_scr.at[0]),
        (kgain_hbm, head_gain_scr.at[1]),
        (mix_gain_hbm, mix_gain_scr),
        (tokens_hbm, tokens_scr),
    ]
    large = [(ffn_gain_hbm, ffn_gain_ref)]
    start = 0
    for source in (wq_hbm, wk_hbm, wv_hbm):
        large.append((source, w_in_ref.at[:, start : start + source.shape[1]]))
        start += source.shape[1]
    large += [
        (w_out_hbm, w_out_ref),
        (key_hbm, key_ref),
    ]
    copies = [
        pltpu.make_async_copy(source, target, sems.at[index])
        for index, (source, target) in enumerate(small + large)
    ]
    for copy in copies:
        copy.start()
    for copy in copies[: len(small)]:
        copy.wait()

    me = lax.axis_index("ep")
    my_gain_ref[...] = mix_gain_scr[pl.ds(me, 1), :]
    own = tokens_scr[...].astype(F32)
    token_scale = lax.rsqrt(jnp.mean(own * own, axis=-1, keepdims=True) + EPSILON)
    scale_ref[...] = jnp.broadcast_to(token_scale, scale_ref.shape)
    for index in range(2):
        head_gain_ref[index : index + 1, :] = jnp.concatenate(
            [head_gain_scr[index]] * KV_HEADS, axis=-1
        )

    column = lax.broadcasted_iota(jnp.int32, (1, tokens * HEADS), 1)
    live = jnp.zeros(column.shape, jnp.int32)
    bias = jnp.zeros(column.shape, F32)
    for token in range(tokens):
        live = jnp.where(column // HEADS == token, lengths_scr[token], live)
    for head in range(HEADS):
        bias = jnp.where(column % HEADS == head, bias_scr[head], bias)
    column_ref[0:1, :] = live.astype(F32)
    column_ref[1:2, :] = bias

    row = lax.broadcasted_iota(jnp.int32, share_ref.shape, 0)
    lane = lax.broadcasted_iota(jnp.int32, share_ref.shape, 1)
    first = jnp.zeros(share_ref.shape, jnp.int32)
    second = jnp.zeros(share_ref.shape, jnp.int32)
    gap = jnp.zeros(share_ref.shape, F32)
    for token in range(tokens):
        first = jnp.where(row == token, routes_scr[0, token], first)
        second = jnp.where(row == token, routes_scr[1, token], second)
        gap = jnp.where(row == token, logits_scr[0, token] - logits_scr[1, token], gap)
    share = jnp.where(first == lane % 64, jax.nn.sigmoid(gap), 0.0)
    share = share + jnp.where(second == lane % 64, jax.nn.sigmoid(-gap), 0.0)
    high = share.astype(BF16).astype(F32)
    share_ref[...] = jnp.where(lane < 64, high, share - high).astype(BF16)
    for copy in copies[len(small) :]:
        copy.wait()


def project_kernel(rows_ref, gain_ref, w_ref, out_ref):
    shards, tokens, width = rows_ref.shape
    rows = rows_ref[...].astype(F32).reshape(shards * tokens, width)
    scaled = (rows * gain_ref[...]).astype(BF16)
    part = jnp.dot(scaled, w_ref[...], preferred_element_type=F32)
    out_ref[...] = part.astype(BF16).reshape(out_ref.shape)


def attend_kernel(
    parts_ref,
    scale_ref,
    column_ref,
    head_gain_ref,
    share_ref,
    key_ref,
    value_hbm,
    row_ref,
    new_key_ref,
    new_value_ref,
    heads_scr,
    value_ref,
    sem,
):
    fetch = pltpu.make_async_copy(value_hbm, value_ref, sem)
    fetch.start()
    shards, tokens, _ = parts_ref.shape
    cache_len = key_ref.shape[1]
    columns = tokens * HEADS

    total = parts_ref[0].astype(F32)
    for shard in range(1, shards):
        total = total + parts_ref[shard].astype(F32)
    total = total * scale_ref[:, 0:1]
    fresh_key = total[:, QUERY_WIDTH : QUERY_WIDTH + KEY_WIDTH]
    new_value_ref[...] = total[:, QUERY_WIDTH + KEY_WIDTH :].astype(BF16)

    lane = lax.broadcasted_iota(jnp.int32, (tokens, KEY_WIDTH), 1)
    squares = fresh_key * fresh_key
    key_scale = jnp.zeros_like(fresh_key)
    for head in range(KV_HEADS):
        mine = lane // HEAD_DIM == head
        mean = jnp.sum(jnp.where(mine, squares, 0.0), axis=-1, keepdims=True) / HEAD_DIM
        key_scale = jnp.where(mine, lax.rsqrt(mean + EPSILON), key_scale)
    new_key_ref[...] = (fresh_key * key_scale * head_gain_ref[1:2, :]).astype(BF16)

    for member in range(GROUP):
        pieces = []
        for group in range(KV_HEADS):
            head = group * GROUP + member
            pieces.append(total[:, head * HEAD_DIM : (head + 1) * HEAD_DIM])
        heads_scr[:, member, :] = jnp.concatenate(pieces, axis=-1)
    stacked = []
    for token in range(tokens):
        stacked += [heads_scr[token]] * KV_HEADS
    query = jnp.concatenate(stacked, axis=0)
    row = lax.broadcasted_iota(jnp.int32, query.shape, 0)
    col = lax.broadcasted_iota(jnp.int32, query.shape, 1)
    query = jnp.where(row % HEADS // GROUP == col // HEAD_DIM, query, 0.0)
    query_mean = jnp.sum(query * query, axis=-1, keepdims=True) / HEAD_DIM
    query = query * lax.rsqrt(query_mean + EPSILON) * head_gain_ref[0:1, :]
    query = query.astype(BF16).astype(F32)
    padded = [
        jnp.where(row // HEADS == token, query, 0.0).astype(BF16) for token in range(tokens)
    ]

    live = column_ref[0:1, :]
    bias = column_ref[1:2, :]
    upper = (
        lax.broadcasted_iota(jnp.int32, (BLOCK, BLOCK), 1)
        >= lax.broadcasted_iota(jnp.int32, (BLOCK, BLOCK), 0)
    ).astype(F32).astype(BF16)
    carry = jnp.zeros((1, columns), F32)
    attended = [jnp.zeros((HEADS, KEY_WIDTH), F32) for _ in range(tokens)]
    for block in range(cache_len // BLOCK - 1, -1, -1):
        span = slice(block * BLOCK, (block + 1) * BLOCK)
        score = lax.dot_general(key_ref[0, span, :], padded[0], NT, preferred_element_type=F32)
        for token in range(1, tokens):
            score = score + lax.dot_general(
                key_ref[token, span, :], padded[token], NT, preferred_element_type=F32
            )
        score = score * HEAD_DIM ** (-0.5) + bias
        spot = lax.broadcasted_iota(jnp.int32, score.shape, 0) + block * BLOCK
        alive = spot.astype(F32) < live
        remain = -(jnp.maximum(score, 0.0) + jnp.log1p(jnp.exp(-jnp.abs(score))))
        remain = jnp.where(alive, remain, 0.0)
        high = remain.astype(BF16)
        low = (remain - high.astype(F32)).astype(BF16)
        inclusive = (
            jnp.dot(upper, high, preferred_element_type=F32)
            + jnp.dot(upper, low, preferred_element_type=F32)
            + carry
        )
        carry = inclusive[0:1, :]
        weight = jnp.where(alive, jnp.exp(score + inclusive), 0.0)
        weight = weight.T.astype(BF16)
        if block == cache_len // BLOCK - 1:
            fetch.wait()
        for token in range(tokens):
            attended[token] = attended[token] + jnp.dot(
                weight[token * HEADS : (token + 1) * HEADS, :],
                value_ref[token, span, :],
                preferred_element_type=F32,
            )

    own_row = lax.broadcasted_iota(jnp.int32, (HEADS, KEY_WIDTH), 0)
    own_col = lax.broadcasted_iota(jnp.int32, (HEADS, KEY_WIDTH), 1)
    keep = own_row // GROUP == own_col // HEAD_DIM
    for token in range(tokens):
        kept = jnp.where(keep, attended[token], 0.0)
        folded = kept[0:GROUP]
        for group in range(1, KV_HEADS):
            folded = folded + kept[group * GROUP : (group + 1) * GROUP]
        heads_scr[token] = folded
    for member in range(GROUP):
        piece = heads_scr[:, member, :].astype(BF16)
        for shard in range(shards):
            row_ref[shard, :, member * KEY_WIDTH : (member + 1) * KEY_WIDTH] = piece

    for shard in range(shards):
        row_ref[shard, :, QUERY_WIDTH:] = share_ref[...]


def mix_kernel(rows_ref, tokens_ref, w_ref, mixed_ref):
    shards, tokens, width = tokens_ref.shape
    total = shards * tokens
    mixed = tokens_ref[...].astype(F32).reshape(total, width)
    rows = rows_ref[...].astype(F32).reshape(total, ROW_WIDTH).astype(BF16)
    for member in range(GROUP):
        pieces = []
        for group in range(KV_HEADS):
            head = group * GROUP + member
            pieces.append(w_ref[head * HEAD_DIM : (head + 1) * HEAD_DIM, :])
        weight = jnp.concatenate(pieces, axis=0)
        mixed = mixed + jnp.dot(
            rows[:, member * KEY_WIDTH : (member + 1) * KEY_WIDTH],
            weight,
            preferred_element_type=F32,
        )
    mixed = mixed.astype(BF16)
    for shard in range(shards):
        mixed_ref[shard] = mixed


def chunk_of(size):
    return BLOCK if size % BLOCK == 0 else size


def expert_kernel(
    mixed_ref,
    rows_ref,
    gain_ref,
    wg_hbm,
    wu_hbm,
    wd_hbm,
    out_ref,
    own_ref,
    wg_ref,
    wu_ref,
    wd_ref,
    sems,
):
    size = wg_ref.shape[1]
    chunk = chunk_of(size)
    steps = size // chunk
    copies = []
    for step in range(steps):
        span = slice(step * chunk, (step + 1) * chunk)
        for index, (source, target) in enumerate(((wg_hbm, wg_ref), (wu_hbm, wu_ref))):
            copies.append(
                pltpu.make_async_copy(
                    source.at[:, span], target.at[:, span], sems.at[index, step]
                )
            )
    for step in range(steps):
        span = slice(step * chunk, (step + 1) * chunk)
        copies.append(
            pltpu.make_async_copy(wd_hbm.at[span, :], wd_ref.at[span, :], sems.at[2, step])
        )
    for copy in copies:
        copy.start()

    total, features = mixed_ref.shape[-2], gain_ref.shape[1]
    shards, tokens = rows_ref.shape[:2]
    if len(mixed_ref.shape) == 3:
        mixed = jnp.concatenate([mixed_ref[s].astype(F32) for s in range(mixed_ref.shape[0])], axis=-1)
    else:
        mixed = mixed_ref[...].astype(F32)
    me = lax.axis_index("ep")
    picked = lax.broadcasted_iota(jnp.int32, (tokens, total), 1) - me * tokens
    picked = picked == lax.broadcasted_iota(jnp.int32, (tokens, total), 0)
    own_ref[...] = jnp.dot(
        picked.astype(F32).astype(BF16), mixed.astype(BF16), preferred_element_type=F32
    )
    scale = lax.rsqrt(jnp.mean(mixed * mixed, axis=-1, keepdims=True) + EPSILON)
    expert_in = (mixed * scale * gain_ref[...]).astype(BF16)
    gates = rows_ref[:, :, QUERY_WIDTH:].astype(F32).reshape(total, 128)
    lane = lax.broadcasted_iota(jnp.int32, gates.shape, 1)
    gate = jnp.where(lane % 64 == me // (FF // size), gates, 0.0)
    gate = jnp.sum(gate, axis=-1, keepdims=True)
    hidden = []
    for step in range(steps):
        span = slice(step * chunk, (step + 1) * chunk)
        copies[2 * step].wait()
        value = jnp.dot(expert_in, wg_ref[:, span], preferred_element_type=F32)
        copies[2 * step + 1].wait()
        up = jnp.dot(expert_in, wu_ref[:, span], preferred_element_type=F32)
        hidden.append((value / (1.0 + jnp.exp(-value)) * up * gate).astype(BF16))
    result = None
    for step in range(steps):
        span = slice(step * chunk, (step + 1) * chunk)
        copies[2 * steps + step].wait()
        part = jnp.dot(hidden[step], wd_ref[span, :], preferred_element_type=F32)
        result = part if result is None else result + part
    out_ref[...] = result.astype(BF16).reshape(out_ref.shape)


def finish_kernel(parts_ref, mixed_ref, out_ref):
    total = mixed_ref[...]
    for shard in range(parts_ref.shape[0]):
        total = total + parts_ref[shard].astype(F32)
    out_ref[...] = total.astype(BF16)


def call(kernel, name, outs, specs, scratch=(), limit=20):
    return pl.pallas_call(
        kernel,
        name=name,
        out_shape=outs,
        in_specs=specs,
        out_specs=jax.tree.map(lambda _: vmem_spec(), outs),
        scratch_shapes=list(scratch),
        compiler_params=pltpu.CompilerParams(vmem_limit_bytes=limit << 20),
    )


def hbm_spec():
    return pl.BlockSpec(memory_space=pltpu.HBM)


def in_hbm(array):
    return pltpu.with_memory_space_constraint(array, pltpu.HBM)


def local(
    tokens,
    lengths,
    cache_key,
    cache_value,
    routes,
    route_logits,
    mix_gain,
    query_gain,
    key_gain,
    head_bias,
    w_query,
    w_key,
    w_value,
    w_out,
    ffn_gain,
    w_gate,
    w_up,
    w_down,
):
    shards = lax.axis_size("ep")
    token_rows, width = tokens.shape
    share = width // shards
    all_rows = shards * token_rows
    exchange = functools.partial(lax.all_to_all, axis_name="ep", split_axis=0, concat_axis=0)
    kept = pltpu.VMEM
    project_width = QUERY_WIDTH + 2 * KEY_WIDTH

    with jax.named_scope("slices"):
        sliced = exchange(tokens.reshape(token_rows, shards, share).transpose(1, 0, 2))
    staged = [
        lengths,
        routes.T,
        route_logits.T,
        head_bias,
        query_gain[None, :],
        key_gain[None, :],
        mix_gain.reshape(shards, share),
        ffn_gain[None, :],
        tokens,
        w_query,
        w_key,
        w_value,
        w_out,
        cache_key,
    ]
    my_gain, scale, column, head_gain, gates, ffn_row, w_in, w_mix, key = call(
        stage_kernel,
        "stage",
        (
            kept((1, share), F32),
            kept((token_rows, 128), F32),
            kept((2, token_rows * HEADS), F32),
            kept((2, KEY_WIDTH), F32),
            kept((token_rows, 128), BF16),
            kept((1, width), F32),
            kept((share, project_width), BF16),
            kept(w_out.shape, BF16),
            kept(cache_key.shape, BF16),
        ),
        [hbm_spec()] * len(staged),
        [
            pltpu.SMEM(lengths.shape, jnp.int32),
            pltpu.SMEM((2, token_rows), jnp.int32),
            pltpu.SMEM((2, token_rows), F32),
            pltpu.SMEM(head_bias.shape, F32),
            pltpu.VMEM((2, 1, HEAD_DIM), F32),
            pltpu.VMEM((shards, share), F32),
            pltpu.VMEM(tokens.shape, BF16),
            pltpu.SemaphoreType.DMA((len(staged),)),
        ],
        limit=4,
    )(*[in_hbm(array) for array in staged])
    parts = call(
        project_kernel,
        "project",
        kept((shards, token_rows, project_width), BF16),
        [vmem_spec()] * 3,
        limit=8,
    )(sliced, my_gain, w_in)
    with jax.named_scope("partial"):
        parts = exchange(parts)

    rows, new_key, new_value = call(
        attend_kernel,
        "attend",
        (
            kept((shards, token_rows, ROW_WIDTH), BF16),
            jax.ShapeDtypeStruct((token_rows, KEY_WIDTH), BF16),
            jax.ShapeDtypeStruct((token_rows, KEY_WIDTH), BF16),
        ),
        [vmem_spec()] * 6 + [hbm_spec()],
        [
            pltpu.VMEM((token_rows, GROUP, KEY_WIDTH), F32),
            pltpu.VMEM(cache_value.shape, BF16),
            pltpu.SemaphoreType.DMA,
        ],
    )(parts, scale, column, head_gain, gates, key, in_hbm(cache_value))
    with jax.named_scope("rows"):
        rows = exchange(rows)

    mixed = call(
        mix_kernel,
        "mix",
        kept((shards, all_rows, share), BF16),
        [vmem_spec()] * 3,
        limit=8,
    )(rows, sliced, w_mix)
    with jax.named_scope("mixed"):
        mixed = exchange(mixed)

    if share % 128:
        expert_rows = mixed.transpose(1, 0, 2).reshape(all_rows, width)
    else:
        expert_rows = mixed
    sums, own = call(
        expert_kernel,
        "expert",
        (kept((shards, token_rows, width), BF16), kept((token_rows, width), F32)),
        [vmem_spec()] * 3 + [hbm_spec()] * 3,
        [
            pltpu.VMEM(w_gate.shape, BF16),
            pltpu.VMEM(w_up.shape, BF16),
            pltpu.VMEM(w_down.shape, BF16),
            pltpu.SemaphoreType.DMA((3, w_gate.shape[1] // chunk_of(w_gate.shape[1]))),
        ],
        limit=40,
    )(expert_rows, rows, ffn_row, in_hbm(w_gate), in_hbm(w_up), in_hbm(w_down))
    with jax.named_scope("sums"):
        sums = exchange(sums)
    output = call(
        finish_kernel,
        "finish",
        jax.ShapeDtypeStruct((token_rows, width), BF16),
        [vmem_spec()] * 2,
        limit=8,
    )(sums, own)
    return output, new_key, new_value


def solution(mesh):
    return jax.shard_map(
        local,
        mesh=mesh,
        in_specs=(
            P(("grp", "ep"), None),
            P(("grp", "ep")),
            P(("grp", "ep"), None, None),
            P(("grp", "ep"), None, None),
            P(("grp", "ep"), None),
            P(("grp", "ep"), None),
            P(),
            P(),
            P(),
            P(),
            P("ep", None),
            P("ep", None),
            P("ep", None),
            P(None, "ep"),
            P(),
            P(None, "ep"),
            P(None, "ep"),
            P("ep", None),
        ),
        out_specs=(P(("grp", "ep"), None), P(("grp", "ep"), None), P(("grp", "ep"), None)),
        check_vma=False,
    )
```

```python
import functools

import jax
import jax.numpy as jnp
from jax import lax
from jax.experimental import pallas as pl
from jax.experimental.pallas import tpu as pltpu
from jax.sharding import PartitionSpec as P


HEADS = 16
KV_HEADS = 4
HEAD_DIM = 64
FF = 7168
EPSILON = 1e-06

GROUP = HEADS // KV_HEADS
KEY_WIDTH = KV_HEADS * HEAD_DIM
QUERY_WIDTH = HEADS * HEAD_DIM
ROW_WIDTH = QUERY_WIDTH + 128
BLOCK = 256
FIRST_HEAD = 1
SECOND_HEAD = 1
F32 = jnp.float32
BF16 = jnp.bfloat16
VMEM = pltpu.VMEM
NT = (((1,), (1,)), ((), ()))


def vmem_spec():
    return pl.BlockSpec(memory_space=VMEM)


def stage_kernel(
    lengths_hbm,
    routes_hbm,
    logits_hbm,
    bias_hbm,
    qgain_hbm,
    kgain_hbm,
    mix_gain_hbm,
    ffn_gain_hbm,
    tokens_hbm,
    wq_hbm,
    wk_hbm,
    wv_hbm,
    w_out_hbm,
    my_gain_ref,
    scale_ref,
    column_ref,
    head_gain_ref,
    share_ref,
    ffn_gain_ref,
    w_in_ref,
    w_out_ref,
    lengths_scr,
    routes_scr,
    logits_scr,
    bias_scr,
    head_gain_scr,
    mix_gain_scr,
    tokens_scr,
    sems,
):
    tokens = tokens_hbm.shape[0]
    small = [
        (lengths_hbm, lengths_scr),
        (routes_hbm, routes_scr),
        (logits_hbm, logits_scr),
        (bias_hbm, bias_scr),
        (qgain_hbm, head_gain_scr.at[0]),
        (kgain_hbm, head_gain_scr.at[1]),
        (mix_gain_hbm, mix_gain_scr),
        (tokens_hbm, tokens_scr),
    ]
    large = [(ffn_gain_hbm, ffn_gain_ref)]
    start = 0
    for source in (wq_hbm, wk_hbm, wv_hbm):
        large.append((source, w_in_ref.at[:, start : start + source.shape[1]]))
        start += source.shape[1]
    large += [
        (w_out_hbm, w_out_ref),
    ]
    copies = [
        pltpu.make_async_copy(source, target, sems.at[index])
        for index, (source, target) in enumerate(small + large)
    ]
    for copy in copies:
        copy.start()
    for copy in copies[: len(small)]:
        copy.wait()

    chip = lax.axis_index("ep") // 2
    my_gain_ref[...] = mix_gain_scr[pl.ds(2 * chip, 2), :]
    own = tokens_scr[...].astype(F32)
    token_scale = lax.rsqrt(jnp.mean(own * own, axis=-1, keepdims=True) + EPSILON)
    scale_ref[...] = jnp.broadcast_to(token_scale, scale_ref.shape)
    for index in range(2):
        head_gain_ref[index : index + 1, :] = jnp.concatenate(
            [head_gain_scr[index]] * KV_HEADS, axis=-1
        )

    column = lax.broadcasted_iota(jnp.int32, (1, tokens * HEADS), 1)
    live = jnp.zeros(column.shape, jnp.int32)
    bias = jnp.zeros(column.shape, F32)
    for token in range(tokens):
        live = jnp.where(column // HEADS == token, lengths_scr[token], live)
    for head in range(HEADS):
        bias = jnp.where(column % HEADS == head, bias_scr[head], bias)
    column_ref[0:1, :] = live.astype(F32)
    column_ref[1:2, :] = bias

    row = lax.broadcasted_iota(jnp.int32, share_ref.shape, 0)
    lane = lax.broadcasted_iota(jnp.int32, share_ref.shape, 1)
    first = jnp.zeros(share_ref.shape, jnp.int32)
    second = jnp.zeros(share_ref.shape, jnp.int32)
    gap = jnp.zeros(share_ref.shape, F32)
    for token in range(tokens):
        first = jnp.where(row == token, routes_scr[0, token], first)
        second = jnp.where(row == token, routes_scr[1, token], second)
        gap = jnp.where(row == token, logits_scr[0, token] - logits_scr[1, token], gap)
    share = jnp.where(first == lane % 64, jax.nn.sigmoid(gap), 0.0)
    share = share + jnp.where(second == lane % 64, jax.nn.sigmoid(-gap), 0.0)
    high = share.astype(BF16).astype(F32)
    share_ref[...] = jnp.where(lane < 64, high, share - high).astype(BF16)
    for copy in copies[len(small) :]:
        copy.wait()


def project_kernel(rows_ref, gain_ref, w_ref, wq_ref, wk_ref, wv_ref, after_ref, out_ref):
    chips, tokens, width = rows_ref.shape
    share = width // 2
    rows = rows_ref[...].astype(F32).reshape(chips * tokens, width)
    first = rows[:, :share] * gain_ref[0:1, :]
    second = rows[:, share:] * gain_ref[1:2, :]
    even = lax.axis_index("ep") % 2 == 0
    own = jnp.where(even, first, second).astype(BF16)
    other = jnp.where(even, second, first).astype(BF16)
    start = 0
    for other_ref in (wq_ref, wk_ref, wv_ref):
        size = other_ref.shape[1]
        span = slice(start, start + size)
        part = jnp.dot(own, w_ref[:, span], preferred_element_type=F32)
        part = part + jnp.dot(other, other_ref[...], preferred_element_type=F32)
        out_ref[:, :, span] = part.astype(BF16).reshape(chips, tokens, size)
        start += size


def attend_kernel(
    heads_of,
    parts_ref,
    scale_ref,
    column_ref,
    head_gain_ref,
    share_ref,
    key_hbm,
    value_hbm,
    wd_hbm,
    *rest,
):
    if heads_of:
        wg_hbm, wu_hbm, wg_ref, wu_ref = *rest[:2], *rest[6:8]
        rest = *rest[2:6], *rest[8:]
    row_ref, new_key_ref, new_value_ref, wd_ref, heads_scr, key_ref, value_ref, sems = rest
    fetches = [
        pltpu.make_async_copy(key_hbm, key_ref, sems.at[0]),
        pltpu.make_async_copy(value_hbm, value_ref, sems.at[1]),
    ]
    pieces = [(wd_hbm, wd_ref)]
    if heads_of:
        pieces += [(wg_hbm.at[:, : wg_ref.shape[1]], wg_ref)]
        pieces += [(wu_hbm.at[:, : wu_ref.shape[1]], wu_ref)]
    later = [
        pltpu.make_async_copy(source, target, sems.at[2 + index])
        for index, (source, target) in enumerate(pieces)
    ]
    for fetch in fetches + later:
        fetch.start()
    shards, tokens, _ = parts_ref.shape
    cache_len = key_ref.shape[1]
    columns = tokens * HEADS

    total = parts_ref[0].astype(F32)
    for shard in range(1, shards):
        total = total + parts_ref[shard].astype(F32)
    total = total * scale_ref[:, 0:1]
    fresh_key = total[:, QUERY_WIDTH : QUERY_WIDTH + KEY_WIDTH]
    new_value_ref[...] = total[:, QUERY_WIDTH + KEY_WIDTH :].astype(BF16)

    lane = lax.broadcasted_iota(jnp.int32, (tokens, KEY_WIDTH), 1)
    squares = fresh_key * fresh_key
    key_scale = jnp.zeros_like(fresh_key)
    for head in range(KV_HEADS):
        mine = lane // HEAD_DIM == head
        mean = jnp.sum(jnp.where(mine, squares, 0.0), axis=-1, keepdims=True) / HEAD_DIM
        key_scale = jnp.where(mine, lax.rsqrt(mean + EPSILON), key_scale)
    new_key_ref[...] = (fresh_key * key_scale * head_gain_ref[1:2, :]).astype(BF16)

    for member in range(GROUP):
        pieces = []
        for group in range(KV_HEADS):
            head = group * GROUP + member
            pieces.append(total[:, head * HEAD_DIM : (head + 1) * HEAD_DIM])
        heads_scr[:, member, :] = jnp.concatenate(pieces, axis=-1)
    stacked = []
    for token in range(tokens):
        stacked += [heads_scr[token]] * KV_HEADS
    query = jnp.concatenate(stacked, axis=0)
    row = lax.broadcasted_iota(jnp.int32, query.shape, 0)
    col = lax.broadcasted_iota(jnp.int32, query.shape, 1)
    query = jnp.where(row % HEADS // GROUP == col // HEAD_DIM, query, 0.0)
    query_mean = jnp.sum(query * query, axis=-1, keepdims=True) / HEAD_DIM
    query = query * lax.rsqrt(query_mean + EPSILON) * head_gain_ref[0:1, :]
    query = query.astype(BF16).astype(F32)
    padded = [
        jnp.where(row // HEADS == token, query, 0.0).astype(BF16) for token in range(tokens)
    ]

    live = column_ref[0:1, :]
    bias = column_ref[1:2, :]
    upper = (
        lax.broadcasted_iota(jnp.int32, (BLOCK, BLOCK), 1)
        >= lax.broadcasted_iota(jnp.int32, (BLOCK, BLOCK), 0)
    ).astype(F32).astype(BF16)
    fetches[0].wait()
    carry = jnp.zeros((1, columns), F32)
    attended = [jnp.zeros((HEADS, KEY_WIDTH), F32) for _ in range(tokens)]
    for block in range(cache_len // BLOCK - 1, -1, -1):
        span = slice(block * BLOCK, (block + 1) * BLOCK)
        score = lax.dot_general(key_ref[0, span, :], padded[0], NT, preferred_element_type=F32)
        for token in range(1, tokens):
            score = score + lax.dot_general(
                key_ref[token, span, :], padded[token], NT, preferred_element_type=F32
            )
        score = score * HEAD_DIM ** (-0.5) + bias
        spot = lax.broadcasted_iota(jnp.int32, score.shape, 0) + block * BLOCK
        alive = spot.astype(F32) < live
        remain = -(jnp.maximum(score, 0.0) + jnp.log1p(jnp.exp(-jnp.abs(score))))
        remain = jnp.where(alive, remain, 0.0)
        high = remain.astype(BF16)
        low = (remain - high.astype(F32)).astype(BF16)
        inclusive = (
            jnp.dot(upper, high, preferred_element_type=F32)
            + jnp.dot(upper, low, preferred_element_type=F32)
            + carry
        )
        carry = inclusive[0:1, :]
        weight = jnp.where(alive, jnp.exp(score + inclusive), 0.0)
        weight = weight.T.astype(BF16)
        if block == cache_len // BLOCK - 1:
            fetches[1].wait()
        for token in range(tokens):
            attended[token] = attended[token] + jnp.dot(
                weight[token * HEADS : (token + 1) * HEADS, :],
                value_ref[token, span, :],
                preferred_element_type=F32,
            )

    own_row = lax.broadcasted_iota(jnp.int32, (HEADS, KEY_WIDTH), 0)
    own_col = lax.broadcasted_iota(jnp.int32, (HEADS, KEY_WIDTH), 1)
    keep = own_row // GROUP == own_col // HEAD_DIM
    for token in range(tokens):
        kept = jnp.where(keep, attended[token], 0.0)
        folded = kept[0:GROUP]
        for group in range(1, KV_HEADS):
            folded = folded + kept[group * GROUP : (group + 1) * GROUP]
        heads_scr[token] = folded
    for member in range(GROUP):
        piece = heads_scr[:, member, :].astype(BF16)
        for shard in range(shards):
            row_ref[shard, :, member * KEY_WIDTH : (member + 1) * KEY_WIDTH] = piece

    for shard in range(shards):
        row_ref[shard, :, QUERY_WIDTH:] = share_ref[...]
    for fetch in later:
        fetch.wait()


def mix_kernel(rows_ref, tokens_ref, own_ref, other_ref, mixed_ref, gate_ref):
    chips, tokens, width = tokens_ref.shape
    total, share = chips * tokens, width // 2
    rows = rows_ref[...].astype(F32).reshape(total, ROW_WIDTH)
    gate_ref[...] = rows[:, QUERY_WIDTH:].astype(BF16)
    rows = rows[:, :QUERY_WIDTH].astype(BF16)
    sides = []
    for w_ref in (own_ref, other_ref):
        side = jnp.zeros((total, share), F32)
        for member in range(GROUP):
            pieces = []
            for group in range(KV_HEADS):
                head = group * GROUP + member
                pieces.append(w_ref[head * HEAD_DIM : (head + 1) * HEAD_DIM, :])
            side = side + jnp.dot(
                rows[:, member * KEY_WIDTH : (member + 1) * KEY_WIDTH],
                jnp.concatenate(pieces, axis=0),
                preferred_element_type=F32,
            )
        sides.append(side)
    even = lax.axis_index("ep") % 2 == 0
    tokens_in = tokens_ref[...].astype(F32).reshape(total, width)
    first = (tokens_in[:, :share] + jnp.where(even, sides[0], sides[1])).astype(BF16)
    second = (tokens_in[:, share:] + jnp.where(even, sides[1], sides[0])).astype(BF16)
    for chip in range(chips):
        mixed_ref[chip, :, :share] = first
        mixed_ref[chip, :, share:] = second


def fetch_kernel(start, after_hbm, gate_hbm, up_hbm, gate_ref, up_ref, sems):
    span = slice(start, start + gate_ref.shape[1])
    copies = [
        pltpu.make_async_copy(gate_hbm.at[:, span], gate_ref, sems.at[0]),
        pltpu.make_async_copy(up_hbm.at[:, span], up_ref, sems.at[1]),
    ]
    for copy in copies:
        copy.start()
    for copy in copies:
        copy.wait()


def chunk_of(size):
    return BLOCK if size % BLOCK == 0 else size


def expert_kernel(
    ready,
    own_mixed_ref,
    other_mixed_ref,
    own_gate_ref,
    other_gate_ref,
    gain_ref,
    wd_ref,
    *rest,
):
    heads = rest[: 2 * ready]
    wg_hbm, wu_hbm, own_ref, other_ref, mine_ref, wg_ref, wu_ref, sems = rest[2 * ready :]
    size = wd_ref.shape[0]
    chunk = chunk_of(size)
    steps = size // chunk
    place_of = {}
    start = 0
    for index in range(ready):
        for offset in range(0, heads[2 * index].shape[1], chunk):
            place_of[start // chunk] = (heads[2 * index], heads[2 * index + 1], offset)
            start += chunk
    copies = {}
    for step in range(start // chunk, steps):
        offset = step * chunk - start
        place_of[step] = (wg_ref, wu_ref, offset)
        for index, (source, target) in enumerate(((wg_hbm, wg_ref), (wu_hbm, wu_ref))):
            copies[index, step] = pltpu.make_async_copy(
                source.at[:, step * chunk : (step + 1) * chunk],
                target.at[:, offset : offset + chunk],
                sems.at[index, step],
            )
    for copy in copies.values():
        copy.start()

    half = own_gate_ref.shape[0]
    tokens = mine_ref.shape[0]
    sides = []
    for mixed_ref in (own_mixed_ref, other_mixed_ref):
        if len(mixed_ref.shape) == 3:
            pieces = [mixed_ref[chip].astype(F32) for chip in range(mixed_ref.shape[0])]
            sides.append(jnp.concatenate(pieces, axis=-1))
        else:
            sides.append(mixed_ref[...].astype(F32))
    me = lax.axis_index("ep")
    picked = lax.broadcasted_iota(jnp.int32, (tokens, half), 1) - me // 2 * tokens
    picked = picked == lax.broadcasted_iota(jnp.int32, (tokens, half), 0)
    mine_ref[...] = jnp.dot(
        picked.astype(F32).astype(BF16), sides[0].astype(BF16), preferred_element_type=F32
    )
    mixed = jnp.concatenate(sides, axis=0)
    scale = lax.rsqrt(jnp.mean(mixed * mixed, axis=-1, keepdims=True) + EPSILON)
    expert_in = (mixed * scale * gain_ref[...]).astype(BF16)
    gates = jnp.concatenate(
        [own_gate_ref[...].astype(F32), other_gate_ref[...].astype(F32)], axis=0
    )
    lane = lax.broadcasted_iota(jnp.int32, gates.shape, 1)
    gate = jnp.where(lane % 64 == me // (FF // size), gates, 0.0)
    gate = jnp.sum(gate, axis=-1, keepdims=True)
    result = None
    for step in range(steps):
        gate_part, up_part, offset = place_of[step]
        if (0, step) in copies:
            copies[0, step].wait()
            copies[1, step].wait()
        value = jnp.dot(
            expert_in, gate_part[:, offset : offset + chunk], preferred_element_type=F32
        )
        up = jnp.dot(
            expert_in, up_part[:, offset : offset + chunk], preferred_element_type=F32
        )
        hidden = (value / (1.0 + jnp.exp(-value)) * up * gate).astype(BF16)
        part = jnp.dot(
            hidden, wd_ref[step * chunk : (step + 1) * chunk, :], preferred_element_type=F32
        )
        result = part if result is None else result + part
    own_ref[...] = result[:half].reshape(own_ref.shape)
    other_ref[...] = result[half:].astype(BF16).reshape(other_ref.shape)


def combine_kernel(own_ref, other_ref, out_ref):
    out_ref[...] = (own_ref[...] + other_ref[...].astype(F32)).astype(BF16)


def finish_kernel(parts_ref, mixed_ref, out_ref):
    total = mixed_ref[...]
    for shard in range(parts_ref.shape[0]):
        total = total + parts_ref[shard].astype(F32)
    out_ref[...] = total.astype(BF16)


def call(kernel, outs, specs, scratch=(), limit=20):
    return pl.pallas_call(
        kernel,
        out_shape=outs,
        in_specs=specs,
        out_specs=jax.tree.map(lambda _: vmem_spec(), outs),
        scratch_shapes=list(scratch),
        compiler_params=pltpu.CompilerParams(vmem_limit_bytes=limit << 20),
    )


def hbm_spec():
    return pl.BlockSpec(memory_space=pltpu.HBM)


def in_hbm(array):
    return pltpu.with_memory_space_constraint(array, pltpu.HBM)


def local(
    tokens,
    lengths,
    cache_key,
    cache_value,
    routes,
    route_logits,
    mix_gain,
    query_gain,
    key_gain,
    head_bias,
    w_query,
    w_key,
    w_value,
    w_out,
    ffn_gain,
    w_gate,
    w_up,
    w_down,
):
    shards = lax.axis_size("ep")
    chips = shards // 2
    token_rows, width = tokens.shape
    share = width // shards
    half_rows = chips * token_rows
    project_width = QUERY_WIDTH + 2 * KEY_WIDTH
    kept = pltpu.VMEM
    groups = [[2 * chip + core for chip in range(chips)] for core in range(2)]
    exchange = functools.partial(
        lax.all_to_all, axis_name="ep", split_axis=0, concat_axis=0, axis_index_groups=groups
    )
    mate = functools.partial(
        lax.ppermute, axis_name="ep", perm=[(index, index ^ 1) for index in range(shards)]
    )

    sliced = exchange(tokens.reshape(token_rows, chips, 2 * share).transpose(1, 0, 2))
    other_in = [mate(w_query), mate(w_key), mate(w_value)]
    other_out = mate(w_out)
    staged = [
        lengths,
        routes.T,
        route_logits.T,
        head_bias,
        query_gain[None, :],
        key_gain[None, :],
        mix_gain.reshape(shards, share),
        ffn_gain[None, :],
        tokens,
        w_query,
        w_key,
        w_value,
        w_out,
    ]
    my_gain, scale, column, head_gain, gates, ffn_row, w_in, w_mix = call(
        stage_kernel,
        (
            kept((2, share), F32),
            kept((token_rows, 128), F32),
            kept((2, token_rows * HEADS), F32),
            kept((2, KEY_WIDTH), F32),
            kept((token_rows, 128), BF16),
            kept((1, width), F32),
            kept((share, project_width), BF16),
            kept(w_out.shape, BF16),
        ),
        [hbm_spec()] * len(staged),
        [
            pltpu.SMEM(lengths.shape, jnp.int32),
            pltpu.SMEM((2, token_rows), jnp.int32),
            pltpu.SMEM((2, token_rows), F32),
            pltpu.SMEM(head_bias.shape, F32),
            pltpu.VMEM((2, 1, HEAD_DIM), F32),
            pltpu.VMEM((shards, share), F32),
            pltpu.VMEM(tokens.shape, BF16),
            pltpu.SemaphoreType.DMA((len(staged),)),
        ],
        limit=4,
    )(*[in_hbm(array) for array in staged])
    parts = call(
        project_kernel,
        kept((chips, token_rows, project_width), BF16),
        [vmem_spec()] * 6 + [pl.BlockSpec(memory_space=pl.ANY)],
        limit=8,
    )(sliced, my_gain, w_in, *other_in, other_out)
    parts = exchange(parts)

    size = w_gate.shape[1]
    chunk = chunk_of(size)
    first_head = min(FIRST_HEAD, size // chunk) * chunk
    second_head = min(SECOND_HEAD * chunk, size - first_head)
    early = [in_hbm(w_gate), in_hbm(w_up)] if first_head else []
    rows, new_key, new_value, wd_all, *heads = call(
        functools.partial(attend_kernel, bool(early)),
        (
            kept((chips, token_rows, ROW_WIDTH), BF16),
            jax.ShapeDtypeStruct((token_rows, KEY_WIDTH), BF16),
            jax.ShapeDtypeStruct((token_rows, KEY_WIDTH), BF16),
            kept(w_down.shape, BF16),
        )
        + tuple(kept((width, first_head), BF16) for _ in early),
        [vmem_spec()] * 5 + [hbm_spec()] * (3 + len(early)),
        [
            pltpu.VMEM((token_rows, GROUP, KEY_WIDTH), F32),
            pltpu.VMEM(cache_key.shape, BF16),
            pltpu.VMEM(cache_value.shape, BF16),
            pltpu.SemaphoreType.DMA((5,)),
        ],
    )(
        parts,
        scale,
        column,
        head_gain,
        gates,
        in_hbm(cache_key),
        in_hbm(cache_value),
        in_hbm(w_down),
        *early,
    )
    rows = exchange(rows)

    mixed, own_gate = call(
        mix_kernel,
        (kept((chips, half_rows, 2 * share), BF16), kept((half_rows, 128), BF16)),
        [vmem_spec()] * 4,
        limit=8,
    )(rows, sliced, w_mix, other_out)
    other_gate = mate(own_gate)
    mixed = exchange(mixed)
    other_mixed = mate(mixed)
    if second_head:
        heads += call(
            functools.partial(fetch_kernel, first_head),
            (kept((width, second_head), BF16), kept((width, second_head), BF16)),
            [pl.BlockSpec(memory_space=pl.ANY)] + [hbm_spec()] * 2,
            [pltpu.SemaphoreType.DMA((2,))],
            limit=4,
        )(mixed, in_hbm(w_gate), in_hbm(w_up))

    if 2 * share % 128:
        both = [side.transpose(1, 0, 2).reshape(half_rows, width) for side in (mixed, other_mixed)]
    else:
        both = [mixed, other_mixed]
    tail = max(size - first_head - second_head, chunk)
    own, other, mine = call(
        functools.partial(expert_kernel, len(heads) // 2),
        (
            kept((chips, token_rows, width), F32),
            kept((chips, token_rows, width), BF16),
            kept((token_rows, width), F32),
        ),
        [vmem_spec()] * (6 + len(heads)) + [hbm_spec()] * 2,
        [
            pltpu.VMEM((width, tail), BF16),
            pltpu.VMEM((width, tail), BF16),
            pltpu.SemaphoreType.DMA((2, size // chunk)),
        ],
        limit=28,
    )(
        *both,
        own_gate,
        other_gate,
        ffn_row,
        wd_all,
        *heads,
        in_hbm(w_gate),
        in_hbm(w_up),
    )
    other = mate(other)
    sums = call(
        combine_kernel,
        kept((chips, token_rows, width), BF16),
        [vmem_spec()] * 2,
        limit=8,
    )(own, other)
    sums = exchange(sums)
    output = call(
        finish_kernel,
        jax.ShapeDtypeStruct((token_rows, width), BF16),
        [vmem_spec()] * 2,
        limit=8,
    )(sums, mine)
    return output, new_key, new_value


def solution(mesh):
    return jax.shard_map(
        local,
        mesh=mesh,
        in_specs=(
            P(("grp", "ep"), None),
            P(("grp", "ep")),
            P(("grp", "ep"), None, None),
            P(("grp", "ep"), None, None),
            P(("grp", "ep"), None),
            P(("grp", "ep"), None),
            P(),
            P(),
            P(),
            P(),
            P("ep", None),
            P("ep", None),
            P("ep", None),
            P(None, "ep"),
            P(),
            P(None, "ep"),
            P(None, "ep"),
            P("ep", None),
        ),
        out_specs=(P(("grp", "ep"), None), P(("grp", "ep"), None), P(("grp", "ep"), None)),
        check_vma=False,
    )
```

```python
import functools

import jax
import jax.numpy as jnp
from jax import lax
from jax.experimental import pallas as pl
from jax.experimental.pallas import tpu as pltpu
from jax.sharding import PartitionSpec as P


HEADS = 16
KV_HEADS = 4
HEAD_DIM = 64
FF = 7168
EPSILON = 1e-06

GROUP = HEADS // KV_HEADS
KEY_WIDTH = KV_HEADS * HEAD_DIM
QUERY_WIDTH = HEADS * HEAD_DIM
BLOCK = 256
FIRST = 2
SECOND = 0
F32 = jnp.float32
BF16 = jnp.bfloat16
VMEM = pltpu.VMEM
NT = (((1,), (1,)), ((), ()))


def vmem_spec():
    return pl.BlockSpec(memory_space=VMEM)


def stage_kernel(
    lengths_hbm,
    routes_hbm,
    logits_hbm,
    bias_hbm,
    qgain_hbm,
    kgain_hbm,
    mix_gain_hbm,
    ffn_gain_hbm,
    tokens_hbm,
    wq_hbm,
    wk_hbm,
    wv_hbm,
    w_out_hbm,
    key_hbm,
    my_gain_ref,
    scale_ref,
    column_ref,
    head_gain_ref,
    share_ref,
    ffn_gain_ref,
    w_in_ref,
    w_out_ref,
    key_ref,
    lengths_scr,
    routes_scr,
    logits_scr,
    bias_scr,
    head_gain_scr,
    mix_gain_scr,
    tokens_scr,
    sems,
):
    tokens = tokens_hbm.shape[0]
    small = [
        (lengths_hbm, lengths_scr),
        (routes_hbm, routes_scr),
        (logits_hbm, logits_scr),
        (bias_hbm, bias_scr),
        (qgain_hbm, head_gain_scr.at[0]),
        (kgain_hbm, head_gain_scr.at[1]),
        (mix_gain_hbm, mix_gain_scr),
        (tokens_hbm, tokens_scr),
    ]
    large = [(ffn_gain_hbm, ffn_gain_ref)]
    start = 0
    for source in (wq_hbm, wk_hbm, wv_hbm):
        large.append((source, w_in_ref.at[:, start : start + source.shape[1]]))
        start += source.shape[1]
    large += [
        (w_out_hbm, w_out_ref),
        (key_hbm, key_ref),
    ]
    copies = [
        pltpu.make_async_copy(source, target, sems.at[index])
        for index, (source, target) in enumerate(small + large)
    ]
    for copy in copies:
        copy.start()
    for copy in copies[: len(small)]:
        copy.wait()

    chip = lax.axis_index("ep") // 2
    my_gain_ref[...] = mix_gain_scr[pl.ds(2 * chip, 2), :]
    own = tokens_scr[...].astype(F32)
    token_scale = lax.rsqrt(jnp.mean(own * own, axis=-1, keepdims=True) + EPSILON)
    scale_ref[...] = jnp.broadcast_to(token_scale, scale_ref.shape)
    for index in range(2):
        head_gain_ref[index : index + 1, :] = jnp.concatenate(
            [head_gain_scr[index]] * KV_HEADS, axis=-1
        )

    columns = tokens * HEADS
    column = lax.broadcasted_iota(jnp.int32, column_ref[0:1, :].shape, 1)
    live = jnp.zeros(column.shape, jnp.int32)
    bias = jnp.zeros(column.shape, F32)
    for token in range(tokens):
        live = jnp.where(column % columns // HEADS == token, lengths_scr[token], live)
    for head in range(HEADS):
        bias = jnp.where(column % HEADS == head, bias_scr[head], bias)
    live = live - jnp.where(column >= columns, key_hbm.shape[1] // 2, 0)
    column_ref[0:1, :] = live.astype(F32)
    column_ref[1:2, :] = bias

    row = lax.broadcasted_iota(jnp.int32, share_ref.shape, 0)
    lane = lax.broadcasted_iota(jnp.int32, share_ref.shape, 1)
    first = jnp.zeros(share_ref.shape, jnp.int32)
    second = jnp.zeros(share_ref.shape, jnp.int32)
    gap = jnp.zeros(share_ref.shape, F32)
    for token in range(tokens):
        first = jnp.where(row == token, routes_scr[0, token], first)
        second = jnp.where(row == token, routes_scr[1, token], second)
        gap = jnp.where(row == token, logits_scr[0, token] - logits_scr[1, token], gap)
    share = jnp.where(first == lane, jax.nn.sigmoid(gap), 0.0)
    share_ref[...] = share + jnp.where(second == lane, jax.nn.sigmoid(-gap), 0.0)
    for copy in copies[len(small) :]:
        copy.wait()


def project_kernel(rows_ref, gain_ref, w_ref, wq_ref, wk_ref, wv_ref, after_ref, out_ref):
    chips, tokens, width = rows_ref.shape
    share = width // 2
    rows = rows_ref[...].astype(F32).reshape(chips * tokens, width)
    first = rows[:, :share] * gain_ref[0:1, :]
    second = rows[:, share:] * gain_ref[1:2, :]
    even = lax.axis_index("ep") % 2 == 0
    own = jnp.where(even, first, second).astype(BF16)
    other = jnp.where(even, second, first).astype(BF16)
    start = 0
    for other_ref in (wq_ref, wk_ref, wv_ref):
        size = other_ref.shape[1]
        span = slice(start, start + size)
        part = jnp.dot(own, w_ref[:, span], preferred_element_type=F32)
        part = part + jnp.dot(other, other_ref[...], preferred_element_type=F32)
        out_ref[:, :, span] = part.astype(BF16).reshape(chips, tokens, size)
        start += size


def weight_copies(places, sems, *sources):
    wg_hbm, wu_hbm, wd_hbm = sources
    size = wd_hbm.shape[0]
    chunk = chunk_of(size)
    copies = {}
    for step, (wg_ref, wu_ref, wd_ref, offset) in places.items():
        span = slice(step * chunk, (step + 1) * chunk)
        place = slice(offset, offset + chunk)
        row = len(copies)
        copies[step] = [
            pltpu.make_async_copy(wg_hbm.at[:, span], wg_ref.at[:, place], sems.at[row, 0]),
            pltpu.make_async_copy(wu_hbm.at[:, span], wu_ref.at[:, place], sems.at[row, 1]),
            pltpu.make_async_copy(wd_hbm.at[span, :], wd_ref.at[place, :], sems.at[row, 2]),
        ]
    return copies


def places_of(first, parts, chunk):
    count = parts[2].shape[0] // chunk
    return {first + index: (*parts, index * chunk) for index in range(count)}


def attend_kernel(
    parts_ref,
    scale_ref,
    column_ref,
    head_gain_ref,
    key_ref,
    value_hbm,
    wg_hbm,
    wu_hbm,
    wd_hbm,
    row_ref,
    new_key_ref,
    new_value_ref,
    wg_ref,
    wu_ref,
    wd_ref,
    heads_scr,
    value_ref,
    sem,
    sems,
):
    fetch = pltpu.make_async_copy(value_hbm, value_ref, sem)
    fetch.start()
    places = places_of(0, (wg_ref, wu_ref, wd_ref), chunk_of(wd_hbm.shape[0]))
    later = sum(weight_copies(places, sems, wg_hbm, wu_hbm, wd_hbm).values(), [])
    for copy in later:
        copy.start()
    shards, tokens, _ = parts_ref.shape
    cache_len = key_ref.shape[1]
    columns = tokens * HEADS

    total = parts_ref[0].astype(F32)
    for shard in range(1, shards):
        total = total + parts_ref[shard].astype(F32)
    total = total * scale_ref[:, 0:1]
    fresh_key = total[:, QUERY_WIDTH : QUERY_WIDTH + KEY_WIDTH]
    new_value_ref[...] = total[:, QUERY_WIDTH + KEY_WIDTH :].astype(BF16)

    lane = lax.broadcasted_iota(jnp.int32, (tokens, KEY_WIDTH), 1)
    squares = fresh_key * fresh_key
    key_scale = jnp.zeros_like(fresh_key)
    for head in range(KV_HEADS):
        mine = lane // HEAD_DIM == head
        mean = jnp.sum(jnp.where(mine, squares, 0.0), axis=-1, keepdims=True) / HEAD_DIM
        key_scale = jnp.where(mine, lax.rsqrt(mean + EPSILON), key_scale)
    new_key_ref[...] = (fresh_key * key_scale * head_gain_ref[1:2, :]).astype(BF16)

    for member in range(GROUP):
        pieces = []
        for group in range(KV_HEADS):
            head = group * GROUP + member
            pieces.append(total[:, head * HEAD_DIM : (head + 1) * HEAD_DIM])
        heads_scr[:, member, :] = jnp.concatenate(pieces, axis=-1)
    stacked = []
    for token in range(tokens):
        stacked += [heads_scr[token]] * KV_HEADS
    query = jnp.concatenate(stacked, axis=0)
    row = lax.broadcasted_iota(jnp.int32, query.shape, 0)
    col = lax.broadcasted_iota(jnp.int32, query.shape, 1)
    query = jnp.where(row % HEADS // GROUP == col // HEAD_DIM, query, 0.0)
    query_mean = jnp.sum(query * query, axis=-1, keepdims=True) / HEAD_DIM
    query = query * lax.rsqrt(query_mean + EPSILON) * head_gain_ref[0:1, :]
    query = query.astype(BF16).astype(F32)
    half = cache_len // 2
    blocks = half // BLOCK
    lower, upper = [], []
    for token in range(tokens):
        mine = jnp.where(row // HEADS == token, query, 0.0)
        lower.append(jnp.concatenate([mine, jnp.zeros_like(mine)], axis=0).astype(BF16))
        upper.append(jnp.concatenate([jnp.zeros_like(mine), mine], axis=0).astype(BF16))
    live = column_ref[0:1, :]
    bias = column_ref[1:2, :]
    after = (
        lax.broadcasted_iota(jnp.int32, (BLOCK, BLOCK), 1)
        >= lax.broadcasted_iota(jnp.int32, (BLOCK, BLOCK), 0)
    ).astype(F32).astype(BF16)
    scores = []
    for block in range(blocks):
        score = None
        for token in range(tokens):
            for start, side in ((0, lower), (half, upper)):
                span = slice(start + block * BLOCK, start + (block + 1) * BLOCK)
                part = lax.dot_general(
                    key_ref[token, span, :], side[token], NT, preferred_element_type=F32
                )
                score = part if score is None else score + part
        scores.append(score * HEAD_DIM ** (-0.5) + bias)
    sums = []
    for block in range(blocks):
        score = scores[block]
        spot = lax.broadcasted_iota(jnp.int32, score.shape, 0) + block * BLOCK
        remain = -(jnp.maximum(score, 0.0) + jnp.log1p(jnp.exp(-jnp.abs(score))))
        remain = jnp.where(spot.astype(F32) < live, remain, 0.0)
        high = remain.astype(BF16)
        low = (remain - high.astype(F32)).astype(BF16)
        sums.append(
            jnp.dot(after, high, preferred_element_type=F32)
            + jnp.dot(after, low, preferred_element_type=F32)
        )
    totals = [part[0:1, :] for part in sums]
    whole = functools.reduce(jnp.add, totals)
    lane = lax.broadcasted_iota(jnp.int32, whole.shape, 1)
    carry = jnp.where(lane < columns, jnp.concatenate([whole[:, columns:]] * 2, axis=-1), 0.0)
    weights = [None] * blocks
    for block in range(blocks - 1, -1, -1):
        score = scores[block]
        spot = lax.broadcasted_iota(jnp.int32, score.shape, 0) + block * BLOCK
        weight = jnp.exp(score + (sums[block] + carry))
        weight = jnp.where(spot.astype(F32) < live, weight, 0.0)
        weights[block] = weight.T.astype(BF16)
        carry = carry + totals[block]
    fetch.wait()
    attended = []
    for token in range(tokens):
        total_of = None
        for block in range(blocks):
            for start, line in ((0, 0), (half, columns)):
                span = slice(start + block * BLOCK, start + (block + 1) * BLOCK)
                first = line + token * HEADS
                part = jnp.dot(
                    weights[block][first : first + HEADS, :],
                    value_ref[token, span, :],
                    preferred_element_type=F32,
                )
                total_of = part if total_of is None else total_of + part
        attended.append(total_of)

    own_row = lax.broadcasted_iota(jnp.int32, (HEADS, KEY_WIDTH), 0)
    own_col = lax.broadcasted_iota(jnp.int32, (HEADS, KEY_WIDTH), 1)
    keep = own_row // GROUP == own_col // HEAD_DIM
    for token in range(tokens):
        kept = jnp.where(keep, attended[token], 0.0)
        folded = kept[0:GROUP]
        for group in range(1, KV_HEADS):
            folded = folded + kept[group * GROUP : (group + 1) * GROUP]
        heads_scr[token] = folded
    for member in range(GROUP):
        piece = heads_scr[:, member, :].astype(BF16)
        for shard in range(shards):
            row_ref[shard, :, member * KEY_WIDTH : (member + 1) * KEY_WIDTH] = piece

    for copy in later:
        copy.wait()


def mix_kernel(rows_ref, tokens_ref, own_ref, other_ref, mixed_ref):
    chips, tokens, width = tokens_ref.shape
    total, share = chips * tokens, width // 2
    rows = rows_ref[...].astype(F32).reshape(total, QUERY_WIDTH)
    rows = rows.astype(BF16)
    sides = []
    for w_ref in (own_ref, other_ref):
        side = jnp.zeros((total, share), F32)
        for member in range(GROUP):
            pieces = []
            for group in range(KV_HEADS):
                head = group * GROUP + member
                pieces.append(w_ref[head * HEAD_DIM : (head + 1) * HEAD_DIM, :])
            side = side + jnp.dot(
                rows[:, member * KEY_WIDTH : (member + 1) * KEY_WIDTH],
                jnp.concatenate(pieces, axis=0),
                preferred_element_type=F32,
            )
        sides.append(side)
    even = lax.axis_index("ep") % 2 == 0
    tokens_in = tokens_ref[...].astype(F32).reshape(total, width)
    first = (tokens_in[:, :share] + jnp.where(even, sides[0], sides[1])).astype(BF16)
    second = (tokens_in[:, share:] + jnp.where(even, sides[1], sides[0])).astype(BF16)
    for chip in range(chips):
        mixed_ref[chip, :, :share] = first
        mixed_ref[chip, :, share:] = second


def fetch_kernel(
    first, after_hbm, wg_hbm, wu_hbm, wd_hbm, wg_ref, wu_ref, wd_ref, sems
):
    places = places_of(first, (wg_ref, wu_ref, wd_ref), chunk_of(wd_hbm.shape[0]))
    copies = sum(weight_copies(places, sems, wg_hbm, wu_hbm, wd_hbm).values(), [])
    for copy in copies:
        copy.start()
    for copy in copies:
        copy.wait()


def chunk_of(size):
    return BLOCK if size % BLOCK == 0 else size


def expert_kernel(ready, own_mixed_ref, other_mixed_ref, gain_ref, *rest):
    heads, rest = rest[: 3 * ready], rest[3 * ready :]
    wg_hbm, wu_hbm, wd_hbm, own_ref, other_ref, mine_ref, *tail, sems = rest
    size = wd_hbm.shape[0]
    chunk = chunk_of(size)
    steps = size // chunk
    places = {}
    for index in range(0, 3 * ready, 3):
        places |= places_of(len(places), heads[index : index + 3], chunk)
    copies = {}
    if len(places) < steps:
        rest_of = places_of(len(places), tail, chunk)
        copies = weight_copies(rest_of, sems, wg_hbm, wu_hbm, wd_hbm)
        places |= rest_of
    for group in copies.values():
        for copy in group[:2]:
            copy.start()
    for group in copies.values():
        group[2].start()

    tokens = mine_ref.shape[0]
    half = own_ref.shape[0] * tokens
    sides = []
    for mixed_ref in (own_mixed_ref, other_mixed_ref):
        if len(mixed_ref.shape) == 3:
            pieces = [mixed_ref[chip].astype(F32) for chip in range(mixed_ref.shape[0])]
            sides.append(jnp.concatenate(pieces, axis=-1))
        else:
            sides.append(mixed_ref[...].astype(F32))
    me = lax.axis_index("ep")
    picked = lax.broadcasted_iota(jnp.int32, (tokens, half), 1) - me // 2 * tokens
    picked = picked == lax.broadcasted_iota(jnp.int32, (tokens, half), 0)
    mine_ref[...] = jnp.dot(
        picked.astype(F32).astype(BF16), sides[0].astype(BF16), preferred_element_type=F32
    )
    mixed = jnp.concatenate(sides, axis=0)
    scale = lax.rsqrt(jnp.mean(mixed * mixed, axis=-1, keepdims=True) + EPSILON)
    expert_in = (mixed * scale * gain_ref[...]).astype(BF16)
    result = None
    held = None
    waiting = []

    def project_down(result):
        for index, (hidden, wd_ref, place) in waiting:
            for copy in copies.get(index, [])[2:]:
                copy.wait()
            part = jnp.dot(hidden, wd_ref[place, :], preferred_element_type=F32)
            result = part if result is None else result + part
        waiting.clear()
        return result

    for step in range(steps + 1):
        fresh = None
        if step < steps:
            wg_ref, wu_ref, wd_ref, offset = places[step]
            place = slice(offset, offset + chunk)
            for copy in copies.get(step, [])[:2]:
                copy.wait()
            value = jnp.dot(expert_in, wg_ref[:, place], preferred_element_type=F32)
            up = jnp.dot(expert_in, wu_ref[:, place], preferred_element_type=F32)
            fresh = value, up, wd_ref, place
        if held is not None:
            value, up, wd_ref, place = held
            hidden = (value / (1.0 + jnp.exp(-value)) * up).astype(BF16)
            waiting.append((step - 1, (hidden, wd_ref, place)))
            if step - 1 not in copies:
                result = project_down(result)
        held = fresh
    result = project_down(result)
    own_ref[...] = result[:half].reshape(own_ref.shape)
    other_ref[...] = result[half:].astype(BF16).reshape(other_ref.shape)


def combine_kernel(own_ref, other_ref, out_ref):
    out_ref[...] = (own_ref[...] + other_ref[...].astype(F32)).astype(BF16)


def finish_kernel(
    size,
    parts_ref,
    gate_ref,
    mixed_ref,
    key_ref,
    value_ref,
    out_ref,
    new_key_ref,
    new_value_ref,
):
    new_key_ref[...] = key_ref[...]
    new_value_ref[...] = value_ref[...]
    total = mixed_ref[...]
    for chip in range(parts_ref.shape[0]):
        expert = 2 * chip // (FF // size)
        total = total + parts_ref[chip].astype(F32) * gate_ref[:, expert : expert + 1]
    out_ref[...] = total.astype(BF16)


def call(kernel, outs, specs, scratch=(), limit=20):
    return pl.pallas_call(
        kernel,
        out_shape=outs,
        in_specs=specs,
        out_specs=jax.tree.map(lambda _: vmem_spec(), outs),
        scratch_shapes=list(scratch),
        compiler_params=pltpu.CompilerParams(vmem_limit_bytes=limit << 20),
    )


def hbm_spec():
    return pl.BlockSpec(memory_space=pltpu.HBM)


def in_hbm(array):
    return pltpu.with_memory_space_constraint(array, pltpu.HBM)


def local(
    tokens,
    lengths,
    cache_key,
    cache_value,
    routes,
    route_logits,
    mix_gain,
    query_gain,
    key_gain,
    head_bias,
    w_query,
    w_key,
    w_value,
    w_out,
    ffn_gain,
    w_gate,
    w_up,
    w_down,
):
    shards = lax.axis_size("ep")
    chips = shards // 2
    token_rows, width = tokens.shape
    share = width // shards
    half_rows = chips * token_rows
    project_width = QUERY_WIDTH + 2 * KEY_WIDTH
    kept = pltpu.VMEM
    groups = [[2 * chip + core for chip in range(chips)] for core in range(2)]
    exchange = functools.partial(
        lax.all_to_all, axis_name="ep", split_axis=0, concat_axis=0, axis_index_groups=groups
    )
    mate = functools.partial(
        lax.ppermute, axis_name="ep", perm=[(index, index ^ 1) for index in range(shards)]
    )

    sliced = exchange(tokens.reshape(token_rows, chips, 2 * share).transpose(1, 0, 2))
    other_in = [mate(w_query), mate(w_key), mate(w_value)]
    other_out = mate(w_out)
    staged = [
        lengths,
        routes.T,
        route_logits.T,
        head_bias,
        query_gain[None, :],
        key_gain[None, :],
        mix_gain.reshape(shards, share),
        ffn_gain[None, :],
        tokens,
        w_query,
        w_key,
        w_value,
        w_out,
        cache_key,
    ]
    my_gain, scale, column, head_gain, gates, ffn_row, w_in, w_mix, key = call(
        stage_kernel,
        (
            kept((2, share), F32),
            kept((token_rows, 128), F32),
            kept((2, 2 * token_rows * HEADS), F32),
            kept((2, KEY_WIDTH), F32),
            kept((token_rows, 128), F32),
            kept((1, width), F32),
            kept((share, project_width), BF16),
            kept(w_out.shape, BF16),
            kept(cache_key.shape, BF16),
        ),
        [hbm_spec()] * len(staged),
        [
            pltpu.SMEM(lengths.shape, jnp.int32),
            pltpu.SMEM((2, token_rows), jnp.int32),
            pltpu.SMEM((2, token_rows), F32),
            pltpu.SMEM(head_bias.shape, F32),
            pltpu.VMEM((2, 1, HEAD_DIM), F32),
            pltpu.VMEM((shards, share), F32),
            pltpu.VMEM(tokens.shape, BF16),
            pltpu.SemaphoreType.DMA((len(staged),)),
        ],
        limit=4,
    )(*[in_hbm(array) for array in staged])
    parts = call(
        project_kernel,
        kept((chips, token_rows, project_width), BF16),
        [vmem_spec()] * 6 + [pl.BlockSpec(memory_space=pl.ANY)],
        limit=8,
    )(sliced, my_gain, w_in, *other_in, other_out)
    parts = exchange(parts)

    size = w_gate.shape[1]
    chunk = chunk_of(size)
    steps = size // chunk
    first = min(FIRST, steps)
    second = min(SECOND, steps - first)
    experts = [in_hbm(w_gate), in_hbm(w_up), in_hbm(w_down)]

    def triple(count, make):
        wide = count * chunk
        return tuple(make(shape, BF16) for shape in ((width, wide), (width, wide), (wide, width)))

    rows, new_key, new_value, *heads = call(
        attend_kernel,
        (
            kept((chips, token_rows, QUERY_WIDTH), BF16),
            kept((token_rows, KEY_WIDTH), BF16),
            kept((token_rows, KEY_WIDTH), BF16),
        )
        + triple(first, kept),
        [vmem_spec()] * 5 + [hbm_spec()] * 4,
        [
            pltpu.VMEM((token_rows, GROUP, KEY_WIDTH), F32),
            pltpu.VMEM(cache_value.shape, BF16),
            pltpu.SemaphoreType.DMA,
            pltpu.SemaphoreType.DMA((first, 3)),
        ],
    )(parts, scale, column, head_gain, key, in_hbm(cache_value), *experts)
    rows = exchange(rows)

    mixed = call(
        mix_kernel,
        kept((chips, half_rows, 2 * share), BF16),
        [vmem_spec()] * 4,
        limit=8,
    )(rows, sliced, w_mix, other_out)
    mixed = exchange(mixed)
    other_mixed = mate(mixed)
    if second:
        heads += call(
            functools.partial(fetch_kernel, first),
            triple(second, kept),
            [pl.BlockSpec(memory_space=pl.ANY)] + [hbm_spec()] * 3,
            [pltpu.SemaphoreType.DMA((second, 3))],
            limit=4,
        )(mixed, *experts)

    if 2 * share % 128:
        both = [side.transpose(1, 0, 2).reshape(half_rows, width) for side in (mixed, other_mixed)]
    else:
        both = [mixed, other_mixed]
    left = max(steps - first - second, 1)
    own, other, mine = call(
        functools.partial(expert_kernel, len(heads) // 3),
        (
            kept((chips, token_rows, width), F32),
            kept((chips, token_rows, width), BF16),
            kept((token_rows, width), F32),
        ),
        [vmem_spec()] * (3 + len(heads)) + [hbm_spec()] * 3,
        [*triple(left, pltpu.VMEM), pltpu.SemaphoreType.DMA((left, 3))],
        limit=28,
    )(*both, ffn_row, *heads, *experts)
    other = mate(other)
    sums = call(
        combine_kernel,
        kept((chips, token_rows, width), BF16),
        [vmem_spec()] * 2,
        limit=8,
    )(own, other)
    sums = exchange(sums)
    key_row = jax.ShapeDtypeStruct((token_rows, KEY_WIDTH), BF16)
    return call(
        functools.partial(finish_kernel, size),
        (jax.ShapeDtypeStruct((token_rows, width), BF16), key_row, key_row),
        [vmem_spec()] * 5,
        limit=8,
    )(sums, gates, mine, new_key, new_value)


def solution(mesh):
    return jax.shard_map(
        local,
        mesh=mesh,
        in_specs=(
            P(("grp", "ep"), None),
            P(("grp", "ep")),
            P(("grp", "ep"), None, None),
            P(("grp", "ep"), None, None),
            P(("grp", "ep"), None),
            P(("grp", "ep"), None),
            P(),
            P(),
            P(),
            P(),
            P("ep", None),
            P("ep", None),
            P("ep", None),
            P(None, "ep"),
            P(),
            P(None, "ep"),
            P(None, "ep"),
            P("ep", None),
        ),
        out_specs=(P(("grp", "ep"), None), P(("grp", "ep"), None), P(("grp", "ep"), None)),
        check_vma=False,
    )
```

```python
import functools

import jax
import jax.numpy as jnp
from jax import lax
from jax.experimental import pallas as pl
from jax.experimental.pallas import tpu as pltpu
from jax.sharding import PartitionSpec as P


HEADS = 16
KV_HEADS = 4
HEAD_DIM = 64
FF = 7168
EPSILON = 1e-06

GROUP = HEADS // KV_HEADS
KEY_WIDTH = KV_HEADS * HEAD_DIM
QUERY_WIDTH = HEADS * HEAD_DIM
BLOCK = 256
FIRST = 2
F32 = jnp.float32
BF16 = jnp.bfloat16
VMEM = pltpu.VMEM
NT = (((1,), (1,)), ((), ()))


def vmem_spec():
    return pl.BlockSpec(memory_space=VMEM)


def stage_kernel(
    lengths_hbm,
    routes_hbm,
    logits_hbm,
    bias_hbm,
    qgain_hbm,
    kgain_hbm,
    mix_gain_hbm,
    ffn_gain_hbm,
    tokens_hbm,
    wq_hbm,
    wk_hbm,
    wv_hbm,
    w_out_hbm,
    key_hbm,
    my_gain_ref,
    scale_ref,
    column_ref,
    head_gain_ref,
    share_ref,
    ffn_gain_ref,
    w_in_ref,
    w_out_ref,
    key_ref,
    lengths_scr,
    routes_scr,
    logits_scr,
    bias_scr,
    head_gain_scr,
    mix_gain_scr,
    tokens_scr,
    sems,
):
    tokens = tokens_hbm.shape[0]
    small = [
        (lengths_hbm, lengths_scr),
        (routes_hbm, routes_scr),
        (logits_hbm, logits_scr),
        (bias_hbm, bias_scr),
        (qgain_hbm, head_gain_scr.at[0]),
        (kgain_hbm, head_gain_scr.at[1]),
        (mix_gain_hbm, mix_gain_scr),
        (tokens_hbm, tokens_scr),
    ]
    large = [(ffn_gain_hbm, ffn_gain_ref)]
    start = 0
    for source in (wq_hbm, wk_hbm, wv_hbm):
        large.append((source, w_in_ref.at[:, start : start + source.shape[1]]))
        start += source.shape[1]
    large += [
        (w_out_hbm, w_out_ref),
        (key_hbm, key_ref),
    ]
    copies = [
        pltpu.make_async_copy(source, target, sems.at[index])
        for index, (source, target) in enumerate(small + large)
    ]
    for copy in copies:
        copy.start()
    for copy in copies[: len(small)]:
        copy.wait()

    chip = lax.axis_index("ep") // 2
    my_gain_ref[...] = mix_gain_scr[pl.ds(2 * chip, 2), :]
    own = tokens_scr[...].astype(F32)
    token_scale = lax.rsqrt(jnp.mean(own * own, axis=-1, keepdims=True) + EPSILON)
    scale_ref[...] = jnp.broadcast_to(token_scale, scale_ref.shape)
    for index in range(2):
        head_gain_ref[index : index + 1, :] = jnp.concatenate(
            [head_gain_scr[index]] * KV_HEADS, axis=-1
        )

    columns = tokens * HEADS
    column = lax.broadcasted_iota(jnp.int32, column_ref[0:1, :].shape, 1)
    live = jnp.zeros(column.shape, jnp.int32)
    bias = jnp.zeros(column.shape, F32)
    for token in range(tokens):
        live = jnp.where(column % columns // HEADS == token, lengths_scr[token], live)
    for head in range(HEADS):
        bias = jnp.where(column % HEADS == head, bias_scr[head], bias)
    live = live - jnp.where(column >= columns, key_hbm.shape[1] // 2, 0)
    column_ref[0:1, :] = live.astype(F32)
    column_ref[1:2, :] = bias

    row = lax.broadcasted_iota(jnp.int32, share_ref.shape, 0)
    lane = lax.broadcasted_iota(jnp.int32, share_ref.shape, 1)
    first = jnp.zeros(share_ref.shape, jnp.int32)
    second = jnp.zeros(share_ref.shape, jnp.int32)
    gap = jnp.zeros(share_ref.shape, F32)
    for token in range(tokens):
        first = jnp.where(row == token, routes_scr[0, token], first)
        second = jnp.where(row == token, routes_scr[1, token], second)
        gap = jnp.where(row == token, logits_scr[0, token] - logits_scr[1, token], gap)
    share = jnp.where(first == lane, jax.nn.sigmoid(gap), 0.0)
    share_ref[...] = share + jnp.where(second == lane, jax.nn.sigmoid(-gap), 0.0)
    for copy in copies[len(small) :]:
        copy.wait()


def project_kernel(rows_ref, gain_ref, w_ref, wq_ref, wk_ref, wv_ref, after_ref, out_ref):
    chips, tokens, width = rows_ref.shape
    share = width // 2
    rows = rows_ref[...].astype(F32).reshape(chips * tokens, width)
    first = rows[:, :share] * gain_ref[0:1, :]
    second = rows[:, share:] * gain_ref[1:2, :]
    even = lax.axis_index("ep") % 2 == 0
    own = jnp.where(even, first, second).astype(BF16)
    other = jnp.where(even, second, first).astype(BF16)
    start = 0
    for other_ref in (wq_ref, wk_ref, wv_ref):
        size = other_ref.shape[1]
        span = slice(start, start + size)
        part = jnp.dot(own, w_ref[:, span], preferred_element_type=F32)
        part = part + jnp.dot(other, other_ref[...], preferred_element_type=F32)
        out_ref[:, :, span] = part.astype(BF16).reshape(chips, tokens, size)
        start += size


def weight_copies(places, sems, *sources):
    wg_hbm, wu_hbm, wd_hbm = sources
    size = wd_hbm.shape[0]
    chunk = chunk_of(size)
    copies = {}
    for step, (wg_ref, wu_ref, wd_ref, offset) in places.items():
        span = slice(step * chunk, (step + 1) * chunk)
        place = slice(offset, offset + chunk)
        row = len(copies)
        copies[step] = [
            pltpu.make_async_copy(wg_hbm.at[:, span], wg_ref.at[:, place], sems.at[row, 0]),
            pltpu.make_async_copy(wu_hbm.at[:, span], wu_ref.at[:, place], sems.at[row, 1]),
            pltpu.make_async_copy(wd_hbm.at[span, :], wd_ref.at[place, :], sems.at[row, 2]),
        ]
    return copies


def places_of(first, parts, chunk):
    count = parts[2].shape[0] // chunk
    return {first + index: (*parts, index * chunk) for index in range(count)}


def attend_kernel(
    parts_ref,
    scale_ref,
    column_ref,
    head_gain_ref,
    key_ref,
    value_hbm,
    wg_hbm,
    wu_hbm,
    wd_hbm,
    row_ref,
    new_key_ref,
    new_value_ref,
    wg_ref,
    wu_ref,
    wd_ref,
    heads_scr,
    value_ref,
    sem,
    sems,
):
    fetch = pltpu.make_async_copy(value_hbm, value_ref, sem)
    fetch.start()
    places = places_of(0, (wg_ref, wu_ref, wd_ref), chunk_of(wd_hbm.shape[0]))
    later = sum(weight_copies(places, sems, wg_hbm, wu_hbm, wd_hbm).values(), [])
    for copy in later:
        copy.start()
    shards, tokens, _ = parts_ref.shape
    cache_len = key_ref.shape[1]
    columns = tokens * HEADS

    total = parts_ref[0].astype(F32)
    for shard in range(1, shards):
        total = total + parts_ref[shard].astype(F32)
    total = total * scale_ref[:, 0:1]
    fresh_key = total[:, QUERY_WIDTH : QUERY_WIDTH + KEY_WIDTH]
    new_value_ref[...] = total[:, QUERY_WIDTH + KEY_WIDTH :].astype(BF16)

    lane = lax.broadcasted_iota(jnp.int32, (tokens, KEY_WIDTH), 1)
    squares = fresh_key * fresh_key
    key_scale = jnp.zeros_like(fresh_key)
    for head in range(KV_HEADS):
        mine = lane // HEAD_DIM == head
        mean = jnp.sum(jnp.where(mine, squares, 0.0), axis=-1, keepdims=True) / HEAD_DIM
        key_scale = jnp.where(mine, lax.rsqrt(mean + EPSILON), key_scale)
    new_key_ref[...] = (fresh_key * key_scale * head_gain_ref[1:2, :]).astype(BF16)

    for member in range(GROUP):
        pieces = []
        for group in range(KV_HEADS):
            head = group * GROUP + member
            pieces.append(total[:, head * HEAD_DIM : (head + 1) * HEAD_DIM])
        heads_scr[:, member, :] = jnp.concatenate(pieces, axis=-1)
    stacked = []
    for token in range(tokens):
        stacked += [heads_scr[token]] * KV_HEADS
    query = jnp.concatenate(stacked, axis=0)
    row = lax.broadcasted_iota(jnp.int32, query.shape, 0)
    col = lax.broadcasted_iota(jnp.int32, query.shape, 1)
    query = jnp.where(row % HEADS // GROUP == col // HEAD_DIM, query, 0.0)
    query_mean = jnp.sum(query * query, axis=-1, keepdims=True) / HEAD_DIM
    query = query * lax.rsqrt(query_mean + EPSILON) * head_gain_ref[0:1, :]
    query = query.astype(BF16).astype(F32)
    half = cache_len // 2
    blocks = half // BLOCK
    lower, upper = [], []
    for token in range(tokens):
        mine = jnp.where(row // HEADS == token, query, 0.0)
        lower.append(jnp.concatenate([mine, jnp.zeros_like(mine)], axis=0).astype(BF16))
        upper.append(jnp.concatenate([jnp.zeros_like(mine), mine], axis=0).astype(BF16))
    live = column_ref[0:1, :]
    bias = column_ref[1:2, :]
    after = (
        lax.broadcasted_iota(jnp.int32, (BLOCK, BLOCK), 1)
        >= lax.broadcasted_iota(jnp.int32, (BLOCK, BLOCK), 0)
    ).astype(F32).astype(BF16)
    scores = []
    for block in range(blocks):
        score = None
        for token in range(tokens):
            for start, side in ((0, lower), (half, upper)):
                span = slice(start + block * BLOCK, start + (block + 1) * BLOCK)
                part = lax.dot_general(
                    key_ref[token, span, :], side[token], NT, preferred_element_type=F32
                )
                score = part if score is None else score + part
        scores.append(score * HEAD_DIM ** (-0.5) + bias)
    sums = []
    for block in range(blocks):
        score = scores[block]
        spot = lax.broadcasted_iota(jnp.int32, score.shape, 0) + block * BLOCK
        remain = -(jnp.maximum(score, 0.0) + jnp.log1p(jnp.exp(-jnp.abs(score))))
        remain = jnp.where(spot.astype(F32) < live, remain, 0.0)
        high = remain.astype(BF16)
        low = (remain - high.astype(F32)).astype(BF16)
        sums.append(
            jnp.dot(after, high, preferred_element_type=F32)
            + jnp.dot(after, low, preferred_element_type=F32)
        )
    totals = [part[0:1, :] for part in sums]
    whole = functools.reduce(jnp.add, totals)
    lane = lax.broadcasted_iota(jnp.int32, whole.shape, 1)
    carry = jnp.where(lane < columns, jnp.concatenate([whole[:, columns:]] * 2, axis=-1), 0.0)
    weights = [None] * blocks
    for block in range(blocks - 1, -1, -1):
        score = scores[block]
        spot = lax.broadcasted_iota(jnp.int32, score.shape, 0) + block * BLOCK
        weight = jnp.exp(score + (sums[block] + carry))
        weight = jnp.where(spot.astype(F32) < live, weight, 0.0)
        weights[block] = weight.T.astype(BF16)
        carry = carry + totals[block]
    fetch.wait()
    attended = []
    for token in range(tokens):
        total_of = None
        for block in range(blocks):
            for start, line in ((0, 0), (half, columns)):
                span = slice(start + block * BLOCK, start + (block + 1) * BLOCK)
                first = line + token * HEADS
                part = jnp.dot(
                    weights[block][first : first + HEADS, :],
                    value_ref[token, span, :],
                    preferred_element_type=F32,
                )
                total_of = part if total_of is None else total_of + part
        attended.append(total_of)

    own_row = lax.broadcasted_iota(jnp.int32, (HEADS, KEY_WIDTH), 0)
    own_col = lax.broadcasted_iota(jnp.int32, (HEADS, KEY_WIDTH), 1)
    keep = own_row // GROUP == own_col // HEAD_DIM
    for token in range(tokens):
        kept = jnp.where(keep, attended[token], 0.0)
        folded = kept[0:GROUP]
        for group in range(1, KV_HEADS):
            folded = folded + kept[group * GROUP : (group + 1) * GROUP]
        heads_scr[token] = folded
    for member in range(GROUP):
        piece = heads_scr[:, member, :].astype(BF16)
        for shard in range(shards):
            row_ref[shard, :, member * KEY_WIDTH : (member + 1) * KEY_WIDTH] = piece

    for copy in later:
        copy.wait()


def mix_kernel(rows_ref, tokens_ref, own_ref, other_ref, mixed_ref):
    chips, tokens, width = tokens_ref.shape
    total, share = chips * tokens, width // 2
    rows = rows_ref[...].astype(F32).reshape(total, QUERY_WIDTH)
    rows = rows.astype(BF16)
    sides = []
    for w_ref in (own_ref, other_ref):
        side = jnp.zeros((total, share), F32)
        for member in range(GROUP):
            pieces = []
            for group in range(KV_HEADS):
                head = group * GROUP + member
                pieces.append(w_ref[head * HEAD_DIM : (head + 1) * HEAD_DIM, :])
            side = side + jnp.dot(
                rows[:, member * KEY_WIDTH : (member + 1) * KEY_WIDTH],
                jnp.concatenate(pieces, axis=0),
                preferred_element_type=F32,
            )
        sides.append(side)
    even = lax.axis_index("ep") % 2 == 0
    tokens_in = tokens_ref[...].astype(F32).reshape(total, width)
    first = (tokens_in[:, :share] + jnp.where(even, sides[0], sides[1])).astype(BF16)
    second = (tokens_in[:, share:] + jnp.where(even, sides[1], sides[0])).astype(BF16)
    for chip in range(chips):
        mixed_ref[chip, :, :share] = first
        mixed_ref[chip, :, share:] = second


def fetch_kernel(start, after_hbm, source_hbm, target_ref, sem):
    span = slice(start, start + target_ref.shape[0])
    copy = pltpu.make_async_copy(source_hbm.at[span, :], target_ref, sem)
    copy.start()
    copy.wait()


def chunk_of(size):
    return BLOCK if size % BLOCK == 0 else size


def expert_kernel(ready, own_mixed_ref, other_mixed_ref, gain_ref, down_ref, *rest):
    heads, rest = rest[: 3 * ready], rest[3 * ready :]
    wg_hbm, wu_hbm, wd_hbm, own_ref, other_ref, mine_ref, *tail, sems = rest
    size = wd_hbm.shape[0]
    chunk = chunk_of(size)
    steps = size // chunk
    places = {}
    for index in range(0, 3 * ready, 3):
        places |= places_of(len(places), heads[index : index + 3], chunk)
    copies = {}
    if len(places) < steps:
        rest_of = places_of(len(places), tail, chunk)
        copies = weight_copies(rest_of, sems, wg_hbm, wu_hbm, wd_hbm)
        places |= rest_of
        fetched = min(rest_of)
        copies[fetched].pop()
    for group in copies.values():
        for copy in group[:2]:
            copy.start()
    for group in copies.values():
        for copy in group[2:]:
            copy.start()

    tokens = mine_ref.shape[0]
    half = own_ref.shape[0] * tokens
    sides = []
    for mixed_ref in (own_mixed_ref, other_mixed_ref):
        if len(mixed_ref.shape) == 3:
            pieces = [mixed_ref[chip].astype(F32) for chip in range(mixed_ref.shape[0])]
            sides.append(jnp.concatenate(pieces, axis=-1))
        else:
            sides.append(mixed_ref[...].astype(F32))
    me = lax.axis_index("ep")
    picked = lax.broadcasted_iota(jnp.int32, (tokens, half), 1) - me // 2 * tokens
    picked = picked == lax.broadcasted_iota(jnp.int32, (tokens, half), 0)
    mine_ref[...] = jnp.dot(
        picked.astype(F32).astype(BF16), sides[0].astype(BF16), preferred_element_type=F32
    )
    mixed = jnp.concatenate(sides, axis=0)
    scale = lax.rsqrt(jnp.mean(mixed * mixed, axis=-1, keepdims=True) + EPSILON)
    expert_in = (mixed * scale * gain_ref[...]).astype(BF16)
    result = None
    held = None
    waiting = []

    def project_down(result):
        for index, (hidden, wd_ref, place) in waiting:
            for copy in copies.get(index, [])[2:]:
                copy.wait()
            part = jnp.dot(hidden, wd_ref[place, :], preferred_element_type=F32)
            result = part if result is None else result + part
        waiting.clear()
        return result

    for step in range(steps + 1):
        fresh = None
        if step < steps:
            wg_ref, wu_ref, wd_ref, offset = places[step]
            place = slice(offset, offset + chunk)
            for copy in copies.get(step, [])[:2]:
                copy.wait()
            value = jnp.dot(expert_in, wg_ref[:, place], preferred_element_type=F32)
            up = jnp.dot(expert_in, wu_ref[:, place], preferred_element_type=F32)
            if len(copies.get(step, [0, 0, 0])) < 3:
                fresh = value, up, down_ref, slice(0, chunk)
            else:
                fresh = value, up, wd_ref, place
        if held is not None:
            value, up, wd_ref, place = held
            hidden = (value / (1.0 + jnp.exp(-value)) * up).astype(BF16)
            waiting.append((step - 1, (hidden, wd_ref, place)))
            if step - 1 not in copies:
                result = project_down(result)
        held = fresh
    result = project_down(result)
    own_ref[...] = result[:half].reshape(own_ref.shape)
    other_ref[...] = result[half:].astype(BF16).reshape(other_ref.shape)


def combine_kernel(own_ref, other_ref, out_ref):
    out_ref[...] = (own_ref[...] + other_ref[...].astype(F32)).astype(BF16)


def finish_kernel(
    size,
    parts_ref,
    gate_ref,
    mixed_ref,
    key_ref,
    value_ref,
    out_ref,
    new_key_ref,
    new_value_ref,
):
    new_key_ref[...] = key_ref[...]
    new_value_ref[...] = value_ref[...]
    total = mixed_ref[...]
    for chip in range(parts_ref.shape[0]):
        expert = 2 * chip // (FF // size)
        total = total + parts_ref[chip].astype(F32) * gate_ref[:, expert : expert + 1]
    out_ref[...] = total.astype(BF16)


def call(kernel, outs, specs, scratch=(), limit=20):
    return pl.pallas_call(
        kernel,
        out_shape=outs,
        in_specs=specs,
        out_specs=jax.tree.map(lambda _: vmem_spec(), outs),
        scratch_shapes=list(scratch),
        compiler_params=pltpu.CompilerParams(vmem_limit_bytes=limit << 20),
    )


def hbm_spec():
    return pl.BlockSpec(memory_space=pltpu.HBM)


def in_hbm(array):
    return pltpu.with_memory_space_constraint(array, pltpu.HBM)


def local(
    tokens,
    lengths,
    cache_key,
    cache_value,
    routes,
    route_logits,
    mix_gain,
    query_gain,
    key_gain,
    head_bias,
    w_query,
    w_key,
    w_value,
    w_out,
    ffn_gain,
    w_gate,
    w_up,
    w_down,
):
    shards = lax.axis_size("ep")
    chips = shards // 2
    token_rows, width = tokens.shape
    share = width // shards
    half_rows = chips * token_rows
    project_width = QUERY_WIDTH + 2 * KEY_WIDTH
    kept = pltpu.VMEM
    groups = [[2 * chip + core for chip in range(chips)] for core in range(2)]
    exchange = functools.partial(
        lax.all_to_all, axis_name="ep", split_axis=0, concat_axis=0, axis_index_groups=groups
    )
    mate = functools.partial(
        lax.ppermute, axis_name="ep", perm=[(index, index ^ 1) for index in range(shards)]
    )

    sliced = exchange(tokens.reshape(token_rows, chips, 2 * share).transpose(1, 0, 2))
    other_in = [mate(w_query), mate(w_key), mate(w_value)]
    other_out = mate(w_out)
    staged = [
        lengths,
        routes.T,
        route_logits.T,
        head_bias,
        query_gain[None, :],
        key_gain[None, :],
        mix_gain.reshape(shards, share),
        ffn_gain[None, :],
        tokens,
        w_query,
        w_key,
        w_value,
        w_out,
        cache_key,
    ]
    my_gain, scale, column, head_gain, gates, ffn_row, w_in, w_mix, key = call(
        stage_kernel,
        (
            kept((2, share), F32),
            kept((token_rows, 128), F32),
            kept((2, 2 * token_rows * HEADS), F32),
            kept((2, KEY_WIDTH), F32),
            kept((token_rows, 128), F32),
            kept((1, width), F32),
            kept((share, project_width), BF16),
            kept(w_out.shape, BF16),
            kept(cache_key.shape, BF16),
        ),
        [hbm_spec()] * len(staged),
        [
            pltpu.SMEM(lengths.shape, jnp.int32),
            pltpu.SMEM((2, token_rows), jnp.int32),
            pltpu.SMEM((2, token_rows), F32),
            pltpu.SMEM(head_bias.shape, F32),
            pltpu.VMEM((2, 1, HEAD_DIM), F32),
            pltpu.VMEM((shards, share), F32),
            pltpu.VMEM(tokens.shape, BF16),
            pltpu.SemaphoreType.DMA((len(staged),)),
        ],
        limit=4,
    )(*[in_hbm(array) for array in staged])
    parts = call(
        project_kernel,
        kept((chips, token_rows, project_width), BF16),
        [vmem_spec()] * 6 + [pl.BlockSpec(memory_space=pl.ANY)],
        limit=8,
    )(sliced, my_gain, w_in, *other_in, other_out)
    parts = exchange(parts)

    size = w_gate.shape[1]
    chunk = chunk_of(size)
    steps = size // chunk
    first = min(FIRST, steps)
    experts = [in_hbm(w_gate), in_hbm(w_up), in_hbm(w_down)]

    def triple(count, make):
        wide = count * chunk
        return tuple(make(shape, BF16) for shape in ((width, wide), (width, wide), (wide, width)))

    rows, new_key, new_value, *heads = call(
        attend_kernel,
        (
            kept((chips, token_rows, QUERY_WIDTH), BF16),
            kept((token_rows, KEY_WIDTH), BF16),
            kept((token_rows, KEY_WIDTH), BF16),
        )
        + triple(first, kept),
        [vmem_spec()] * 5 + [hbm_spec()] * 4,
        [
            pltpu.VMEM((token_rows, GROUP, KEY_WIDTH), F32),
            pltpu.VMEM(cache_value.shape, BF16),
            pltpu.SemaphoreType.DMA,
            pltpu.SemaphoreType.DMA((first, 3)),
        ],
    )(parts, scale, column, head_gain, key, in_hbm(cache_value), *experts)
    rows = exchange(rows)

    mixed = call(
        mix_kernel,
        kept((chips, half_rows, 2 * share), BF16),
        [vmem_spec()] * 4,
        limit=8,
    )(rows, sliced, w_mix, other_out)
    mixed = exchange(mixed)
    other_mixed = mate(mixed)
    down = call(
        functools.partial(fetch_kernel, min(first, steps - 1) * chunk),
        kept((chunk, width), BF16),
        [pl.BlockSpec(memory_space=pl.ANY), hbm_spec()],
        [pltpu.SemaphoreType.DMA],
        limit=4,
    )(mixed, experts[2])

    if 2 * share % 128:
        both = [side.transpose(1, 0, 2).reshape(half_rows, width) for side in (mixed, other_mixed)]
    else:
        both = [mixed, other_mixed]
    left = max(steps - first, 1)
    own, other, mine = call(
        functools.partial(expert_kernel, len(heads) // 3),
        (
            kept((chips, token_rows, width), F32),
            kept((chips, token_rows, width), BF16),
            kept((token_rows, width), F32),
        ),
        [vmem_spec()] * (4 + len(heads)) + [hbm_spec()] * 3,
        [*triple(left, pltpu.VMEM), pltpu.SemaphoreType.DMA((left, 3))],
        limit=28,
    )(*both, ffn_row, down, *heads, *experts)
    other = mate(other)
    sums = call(
        combine_kernel,
        kept((chips, token_rows, width), BF16),
        [vmem_spec()] * 2,
        limit=8,
    )(own, other)
    sums = exchange(sums)
    key_row = jax.ShapeDtypeStruct((token_rows, KEY_WIDTH), BF16)
    return call(
        functools.partial(finish_kernel, size),
        (jax.ShapeDtypeStruct((token_rows, width), BF16), key_row, key_row),
        [vmem_spec()] * 5,
        limit=8,
    )(sums, gates, mine, new_key, new_value)


def solution(mesh):
    return jax.shard_map(
        local,
        mesh=mesh,
        in_specs=(
            P(("grp", "ep"), None),
            P(("grp", "ep")),
            P(("grp", "ep"), None, None),
            P(("grp", "ep"), None, None),
            P(("grp", "ep"), None),
            P(("grp", "ep"), None),
            P(),
            P(),
            P(),
            P(),
            P("ep", None),
            P("ep", None),
            P("ep", None),
            P(None, "ep"),
            P(),
            P(None, "ep"),
            P(None, "ep"),
            P("ep", None),
        ),
        out_specs=(P(("grp", "ep"), None), P(("grp", "ep"), None), P(("grp", "ep"), None)),
        check_vma=False,
    )
```
